512 devices in a mesh: sp: 32 (over z, x), tp: 16 (over y, core).
Axes of the slice: x: 4, y: 8, z: 8, core: 2. Of those that a mesh axis runs over, the one named last changes fastest.
Arguments:
- outer_gate: bfloat16 [512, 12288], P('tp', 'sp'), may hold values from -6 to 6
- inner_gate: bfloat16 [512, 12288], P('tp', 'sp'), may hold values from -6 to 6
- conv_input: bfloat16 [512, 12288], P('tp', 'sp'), may hold values from -6 to 6
- conv_taps: bfloat16 [3, 512], P(None, 'tp'), may hold values from -3.5 to 3.5
- mix_weight: bfloat16 [512, 2048], P(None, 'tp'), may hold values from -0.25 to 0.25
- residual: bfloat16 [12288, 2048], P('sp', 'tp'), may hold values from -24 to 24
- norm_gain: bfloat16 [2048], P('tp'), may hold values from 0.099609375 to 1.8984375
- routes: int32 [12288, 2], P('sp'), may hold values from 0 to 63, all different within a row; in each aligned block of 384 rows (0 to 383, 384 to 767, ...) at most 24 rows name the same one
- route_scores: float32 [12288, 2], P('sp'), may hold values from 0.05 to 1
- expert_gate: bfloat16 [64, 2048, 2048], P('sp', None, 'tp'), may hold values from -0.125 to 0.125
- expert_up: bfloat16 [64, 2048, 2048], P('sp', None, 'tp'), may hold values from -0.125 to 0.125
- expert_down: bfloat16 [64, 2048, 2048], P('sp', None, 'tp'), may hold values from -0.125 to 0.125
- shared_gate: bfloat16 [2048, 512], P(None, 'tp'), may hold values from -0.125 to 0.125
- shared_up: bfloat16 [2048, 512], P(None, 'tp'), may hold values from -0.125 to 0.125
- shared_down: bfloat16 [512, 2048], P(None, 'tp'), may hold values from -0.25 to 0.25
Outputs:
- layer_out: bfloat16 [12288, 2048], P('sp', 'tp')
The draws below stay inside these ranges and needn't reach their ends.
Inputs may be any that keep to these rules, and one draw needn't show every extreme that they name: `routes`: within the rows of one index of sp (384 tokens), no expert is named by more than 24 of the token and choice pairs, a bound that some block reaches; the experts of one token differ.
All inputs are finite; a program needn't handle non-finite values.
Results may differ from the reference program's by a relative error of at most 0.014.
Values may be sent and summed in bfloat16 or wider, within the bound.
No kernel may reach another device: no remote copies, remote signals or barrier semaphores. Data moves between devices by JAX's collectives and lax.ppermute only.
A program may use at most 64 MiB of HBM per device.

```python
import math
import jax
import jax.numpy as jnp
import numpy as np
from jax import lax

D = 2048
CH = 512
FF = 2048
FS = 512
TOPK = 2
TOK_SP = 384
TOKENS = 12288
EXPERTS = 64
CAP = 24
N_SP = 32


def draw_residual(key, part):
    column = jnp.arange(D, dtype=jnp.float32) / (D - 1)
    column_scale = 0.5 * jnp.exp(column * math.log(6.0))
    values = jnp.clip(jax.random.normal(key, (TOKENS, D), jnp.float32), -6.0, 6.0)
    return (values * column_scale[None, :]).astype(jnp.bfloat16)


def shard_levels(own_key, extent, pieces, least, largest):
    def one(dim, shards_of):
        steps = jax.random.uniform(jax.random.fold_in(jax.random.fold_in(own_key, 6), dim), (shards_of,), jnp.float32, least / len(pieces), largest / len(pieces))
        return jnp.repeat(jnp.exp(steps), extent[dim] // shards_of).reshape((-1,) + (1,) * (len(extent) - dim - 1))

    gain = one(*pieces[0])
    for cut in pieces[1:]:
        gain = gain * one(*cut)
    return gain


def routed_block(rng, own, number, rows, amount, top, limit, slope):
    ranking = jax.random.permutation(rng, amount)
    packed, usual = portions_of(amount, rows * top, limit, slope, True), portions_of(amount, rows * top, limit, slope, False)
    places = jnp.arange(amount)

    def named(tallies, offset_by):
        used = int((tallies > 0).sum())
        fixed = max(1, used // 4)
        passed = fixed + (places - fixed + offset_by * (used - fixed)) % max(1, amount - fixed)
        return jnp.zeros((amount,), jnp.int32).at[ranking[jnp.where(places < fixed, places, passed)]].set(jnp.asarray(tallies, jnp.int32))

    tallies = jnp.where(number % 4 == 0, named(packed, number // 4), named(usual, number - number // 4 - 1))
    mixed = jax.random.permutation(jax.random.fold_in(own, 3), amount)
    donor, receiver = mixed[0:amount // 2 * 2:2], mixed[1:amount // 2 * 2:2]
    slack = jnp.minimum(tallies[donor] - 1, limit - tallies[receiver]) // 2
    slack = jnp.where((donor == ranking[0]) | (receiver == ranking[0]) | (tallies[receiver] == 0), 0, jnp.maximum(slack, 0))
    passed = jax.random.randint(jax.random.fold_in(own, 4), (amount // 2,), 0, 1 << 20) % (slack + 1)
    tallies = tallies.at[donor].add(-passed).at[receiver].add(passed)
    members = jnp.searchsorted(jnp.cumsum(tallies), jnp.arange(rows * top), side="right").astype(jnp.int32)
    listing = members.reshape(top, rows).T
    listing = listing[jax.random.permutation(jax.random.fold_in(own, 1), rows)]
    offset_by = jax.random.randint(jax.random.fold_in(own, 2), (rows, 1), 0, top)
    return jnp.take_along_axis(listing, (jnp.arange(top)[None, :] + offset_by) % top, axis=1)


def portions_of(amount, total, limit, slope, full):
    weights = [(1 << 20) // math.isqrt(standing ** slope) + 1 for standing in range(1, amount + 1)]
    largest = limit if full else min(limit, max(-(-total // amount), total * weights[0] // sum(weights)))
    least = 1 if total - largest >= amount - 1 else 0
    given, spare = [largest] + [least] * (amount - 1), total - largest - least * (amount - 1)
    while spare > 0:
        candidates = [i for i in range(1, amount) if given[i] < largest] or [i for i in range(1, amount) if given[i] < limit]
        whole, remaining = sum([weights[i] for i in candidates]), spare
        for i in candidates:
            extra = min(limit - given[i], max(1, remaining * weights[i] // whole), spare)
            given[i] = given[i] + extra
            spare = spare - extra
    return np.array(given)


def bell_draw(rng, extent, deviation, most, shards=(), kind=jnp.bfloat16):
    array = jax.random.normal(rng, extent, jnp.float32) * deviation
    if len(shards) > 0:
        array = shard_levels(rng, extent, shards, -0.22, 0.18) * array
    return jnp.clip(array, min=-most, max=most).astype(kind)


def setup_inputs(seed: int = 0) -> dict:
    seeds = jax.random.split(jax.random.key(seed), 16)
    outer_gate = bell_draw(seeds[0], (CH, TOKENS), 1.0, 6.0, ((0, 16), (1, 32)))
    inner_gate = bell_draw(seeds[1], (CH, TOKENS), 1.0, 6.0, ((0, 16), (1, 32)))
    conv_input = bell_draw(seeds[2], (CH, TOKENS), 1.0, 6.0, ((0, 16), (1, 32)))
    conv_taps = bell_draw(seeds[3], (3, CH), 3 ** -0.5, 3.5, ((1, 16),))
    mix_weight = bell_draw(seeds[4], (CH, D), CH ** -0.5, 0.25, ((1, 16),))
    residual = draw_residual(jax.random.fold_in(seeds[15], 71), 0)
    norm_gain = jnp.clip(1.0 + 0.18 * jax.random.normal(seeds[6], (D,), jnp.float32), 0.099609375, 1.8984375).astype(jnp.bfloat16)
    routes_keys = jax.random.split(jax.random.fold_in(seeds[7], 1), TOKENS // TOK_SP)
    routes_turns = jax.random.permutation(jax.random.fold_in(seeds[7], 3), TOKENS // TOK_SP)
    routes = jax.vmap(lambda own, number: routed_block(jax.random.fold_in(seeds[7], 2), own, number, TOK_SP, EXPERTS, TOPK, CAP, 2))(routes_keys, routes_turns).reshape((TOKENS, TOPK))
    route_scores = jnp.clip(0.05 + 0.95 * jax.random.uniform(seeds[8], (TOKENS, TOPK), jnp.float32) ** shard_levels(seeds[8], (TOKENS, TOPK), ((0, 32),), -0.2, 0.2), 0.05, 1.0)
    expert_gate = bell_draw(seeds[9], (EXPERTS, D, FF), D ** -0.5, 0.125, ((0, 32), (2, 16)))
    expert_up = bell_draw(seeds[10], (EXPERTS, D, FF), D ** -0.5, 0.125, ((0, 32), (2, 16)))
    expert_down = bell_draw(seeds[11], (EXPERTS, FF, D), FF ** -0.5, 0.125, ((0, 32), (2, 16)))
    shared_gate = bell_draw(seeds[12], (D, FS), D ** -0.5, 0.125, ((1, 16),))
    shared_up = bell_draw(seeds[13], (D, FS), D ** -0.5, 0.125, ((1, 16),))
    shared_down = bell_draw(seeds[14], (FS, D), FS ** -0.5, 0.25, ((1, 16),))
    return {"outer_gate": outer_gate, "inner_gate": inner_gate, "conv_input": conv_input, "conv_taps": conv_taps, "mix_weight": mix_weight, "residual": residual, "norm_gain": norm_gain, "routes": routes, "route_scores": route_scores, "expert_gate": expert_gate, "expert_up": expert_up, "expert_down": expert_down, "shared_gate": shared_gate, "shared_up": shared_up, "shared_down": shared_down}


epsilon = 1e-06
routed_scale = 2.5

def slot_tables(routes_block, expert_count, capacity):
    count_rows, top_count = routes_block.shape
    flat_route = routes_block.reshape(-1)
    onehot = (flat_route[:, None] == jnp.arange(expert_count, dtype=jnp.int32)[None, :]).astype(jnp.int32)
    before = jnp.cumsum(onehot, axis=0) - onehot
    position = lax.optimization_barrier(jnp.sum(before * onehot, axis=1)).astype(jnp.int32)
    slot_index = (flat_route * capacity + position).astype(jnp.int32)
    token_ids = (jnp.arange(count_rows * top_count, dtype=jnp.int32) // top_count).astype(jnp.int32)
    owners = jnp.full((expert_count * capacity,), -1, jnp.int32).at[slot_index].set(token_ids)
    return (slot_index.reshape(count_rows, top_count), owners)

def reference(outer_gate, inner_gate, conv_input, conv_taps, mix_weight, residual, norm_gain, routes, route_scores, expert_gate, expert_up, expert_down, shared_gate, shared_up, shared_down):
    product = (inner_gate.astype(jnp.float32) * conv_input.astype(jnp.float32)).astype(jnp.bfloat16)
    padded = jnp.pad(product.astype(jnp.float32), ((0, 0), (1, 1)))
    kernel = conv_taps.astype(jnp.float32)
    filtered = kernel[0][:, None] * padded[:, :-2] + kernel[1][:, None] * padded[:, 1:-1] + kernel[2][:, None] * padded[:, 2:]
    mixed = (outer_gate.astype(jnp.float32) * filtered).astype(jnp.bfloat16)
    projected = lax.dot_general(mixed, mix_weight, (((0,), (0,)), ((), ())), preferred_element_type=jnp.float32)
    stream = (residual.astype(jnp.float32) + projected).astype(jnp.bfloat16)
    levels = stream.astype(jnp.float32)
    inverse_rms = lax.rsqrt(lax.optimization_barrier(jnp.mean(levels * levels, axis=1)) + epsilon)
    normed = (levels * inverse_rms[:, None] * norm_gain.astype(jnp.float32)).astype(jnp.bfloat16)
    shared_act = (jax.nn.silu(jnp.dot(normed, shared_gate, preferred_element_type=jnp.float32)) * jnp.dot(normed, shared_up, preferred_element_type=jnp.float32)).astype(jnp.bfloat16)
    shared_out = jnp.dot(shared_act, shared_down, preferred_element_type=jnp.float32)
    blocks = routes.reshape(N_SP, TOK_SP, TOPK)
    slot_index, owners = jax.vmap(lambda block: slot_tables(block, EXPERTS, CAP))(blocks)
    offsets = (jnp.arange(N_SP, dtype=jnp.int32) * TOK_SP)[:, None]
    global_rows = jnp.where(owners >= 0, owners + offsets, -1).astype(jnp.int32)
    per_expert = global_rows.reshape(N_SP, EXPERTS, CAP).transpose(1, 0, 2).reshape(EXPERTS, N_SP * CAP)

    def run_expert(inputs):
        row_ids, gate_w, up_w, down_w = inputs
        filled = row_ids >= 0
        rows = jnp.where(filled[:, None], normed[jnp.maximum(row_ids, 0)], jnp.zeros((), jnp.bfloat16))
        gate_act = jnp.dot(rows, gate_w, preferred_element_type=jnp.float32)
        up_act = jnp.dot(rows, up_w, preferred_element_type=jnp.float32)
        hidden = (jax.nn.silu(gate_act) * up_act).astype(jnp.bfloat16)
        return jnp.dot(hidden, down_w, preferred_element_type=jnp.float32).astype(jnp.bfloat16)
    results = lax.map(run_expert, (per_expert, expert_gate, expert_up, expert_down))
    flat_results = results.reshape(EXPERTS * N_SP * CAP, D)
    chosen = routes.reshape(N_SP, TOK_SP, TOPK)
    position = slot_index - chosen * CAP
    block_ids = jnp.arange(N_SP, dtype=jnp.int32)[:, None, None]
    lookup = ((chosen * N_SP + block_ids) * CAP + position).astype(jnp.int32).reshape(TOKENS, TOPK)
    picked = flat_results[lookup].astype(jnp.float32)
    weights = route_scores / lax.optimization_barrier(jnp.sum(route_scores, axis=1, keepdims=True)) * routed_scale
    routed = lax.optimization_barrier(jnp.sum(weights[:, :, None] * picked, axis=1))
    return (stream.astype(jnp.float32) + routed + shared_out).astype(jnp.bfloat16)
```

```python
import jax
import jax.numpy as jnp
from jax import lax
from jax.experimental import pallas as pl
from jax.experimental.pallas import tpu as pltpu
from jax.sharding import Mesh, PartitionSpec as P


epsilon = 1e-06
routed_scale = 2.5
bf16, f32, i32 = jnp.bfloat16, jnp.float32, jnp.int32

D = 2048
TOK = 384
CAP = 24
SP = 32
EXPERTS = 64
HALF = SP // 2 * CAP
SHARE = TOK // 4
GAIN = 8
USED = HALF + SHARE
BLOCK = USED + GAIN
HROWS = HALF + SHARE // 4

NEAR = [(2 * y, 2 * (y ^ 1)) for y in range(8)] + [
    (2 * y + 1, 2 * ((y + (1 if y % 2 else 7)) % 8) + 1) for y in range(8)
]
DOWN = 2 * D
PACK = 3 * D
SDOWN = PACK + D // 2
WROWS = SDOWN + 512

VM = pl.BlockSpec(memory_space=pltpu.VMEM)
ANY = pl.BlockSpec(memory_space=pl.ANY)
MIB = 1 << 20


def dot(a, b):
    return lax.dot_general(a, b, (((1,), (0,)), ((), ())), preferred_element_type=f32)


def call(body, outs, count, scratch=(), limit=8, space=VM):
    return pl.pallas_call(
        body,
        out_shape=outs,
        in_specs=[space] * count,
        out_specs=jax.tree.map(lambda _: space, outs),
        scratch_shapes=scratch,
        compiler_params=pltpu.CompilerParams(vmem_limit_bytes=limit * MIB),
    )


def index(axis):
    return lax.axis_index(axis)


def pick_body(gate, up, down, sg, su, sd, own, other, pack, sem):
    yl = index("yl")
    copies = [
        (w.at[which], out.at[pl.ds(i * D, D)])
        for out, which in ((other, 1 - yl), (own, yl))
        for i, w in enumerate((gate, up, down))
    ] + [(sd, out.at[pl.ds(SDOWN, 512)]) for out in (other, own)]
    copies = [pltpu.make_async_copy(a, b, sem.at[i]) for i, (a, b) in enumerate(copies)]
    loads = [
        pltpu.make_async_copy(
            w.at[:, pl.ds(128 * b, 128)], pack.at[pl.ds(64 * b + 32 * i, 32)], sem.at[8 + 16 * i + b]
        )
        for i, w in enumerate((sg, su))
        for b in range(16)
    ]
    for copy in loads + copies:
        copy.start()
    for copy in loads:
        copy.wait()
    stores = [
        pltpu.make_async_copy(pack, out.at[pl.ds(PACK, D // 2)], sem.at[40 + i])
        for i, out in enumerate((own, other))
    ]
    for copy in stores:
        copy.start()
    for copy in copies + stores:
        copy.wait()


def mixer_body(outer, inner, conv, taps, before, after, out):
    product = (inner[...].astype(f32) * conv[...].astype(f32)).astype(bf16).astype(f32)
    lane = lax.broadcasted_iota(i32, product.shape, 1)
    left = jnp.where(lane == 0, before[...].astype(f32), pltpu.roll(product, 1, 1))
    right = jnp.where(lane == TOK - 1, after[...].astype(f32), pltpu.roll(product, TOK - 1, 1))
    i = lax.broadcasted_iota(i32, (32, 32), 0)
    j = lax.broadcasted_iota(i32, (32, 32), 1)
    k = taps[...].astype(f32)
    k = [jnp.sum(jnp.where(i == j, k[n : n + 1, :], 0.0), axis=1, keepdims=True) for n in range(3)]
    filtered = k[0] * left + k[1] * product + k[2] * right
    out[...] = (outer[...].astype(f32) * filtered).astype(bf16)


def stream_body(mixed, weight, residual, gain, out):
    projected = lax.dot_general(
        mixed[...], weight[...], (((0,), (0,)), ((), ())), preferred_element_type=f32
    )
    out[0:TOK, :] = (residual[...].astype(f32) + projected).astype(bf16)
    out[TOK : TOK + GAIN, :] = jnp.broadcast_to(gain[...], (GAIN, 128))


def meta_body(routes, scores, rows_out, cols_out):
    yl = index("yl")
    e = lax.broadcasted_iota(i32, (EXPERTS, TOK), 0)
    m0 = e == routes[0:1, :]
    m1 = e == routes[1:2, :]
    member = jnp.where(m0 | m1, 1.0, 0.0).astype(bf16)
    a = lax.broadcasted_iota(i32, (TOK, TOK), 0)
    b = lax.broadcasted_iota(i32, (TOK, TOK), 1)
    earlier = dot(member, jnp.where(a < b, 1.0, 0.0).astype(bf16))
    base = (lax.shift_right_logical(e, 1) * CAP + 1).astype(f32)
    value = jnp.where((e & 1) == yl, base + earlier, 0.0)
    s0 = jnp.sum(jnp.where(m0, value, 0.0), axis=0, keepdims=True) - 1.0
    s1 = jnp.sum(jnp.where(m1, value, 0.0), axis=0, keepdims=True) - 1.0
    row = lax.broadcasted_iota(i32, (8, TOK), 0)
    rows_out[...] = jnp.where(row == 0, s0, s1)
    total = scores[0:1, :] + scores[1:2, :]
    w0 = scores[0:1, :] / total * routed_scale
    w1 = scores[1:2, :] / total * routed_scale
    row = lax.broadcasted_iota(i32, (128, TOK), 0)
    table = jnp.where(row == 0, s0, jnp.where(row == 1, s1, jnp.where(row == 2, w0, w1)))
    cols_out[...] = table.T


def dispatch_body(aug, near, slots, send, shared):
    yl = index("yl")
    tokens = jnp.concatenate([aug[0:TOK, :], near[0:TOK, :]], axis=1)
    row = lax.broadcasted_iota(i32, (SP * CAP, TOK), 0).astype(f32)
    pick = (row == slots[0:1, :]) | (row == slots[1:2, :])
    send[...] = dot(jnp.where(pick, 1.0, 0.0).astype(bf16), tokens).astype(bf16)
    for core in range(2):
        start = pl.multiple_of((yl * 2 + core) * SHARE, SHARE)
        for h, x in enumerate((aug, near)):
            lanes = slice(128 * h, 128 * h + 128)
            shared[core, 0:SHARE, lanes] = x[pl.ds(start, SHARE), :]
            shared[core, SHARE : SHARE + GAIN, lanes] = x[TOK : TOK + GAIN, :]


def silu(v):
    return v * (1.0 / (1.0 + jnp.exp(-v)))


def placed(own, up, down, up2, down2):
    yh, yl = index("yh"), index("yl")
    return (
        (2 * yh + yl, own.at[0], own.at[1]),
        (2 * ((yh + 3) % 4) + yl, up.at[0], up.at[1]),
        (2 * ((yh + 1) % 4) + yl, down.at[0], down.at[1]),
        (2 * ((yh + 2) % 4) + yl, up2.at[0], down2.at[0]),
    )


def slice_of(y, core, near):
    if near:
        yl = index("yl")
        y = (y + 2 * yl + 7) % 8 if core else y + 1 - 2 * yl
    return 2 * y + core


def up_body(*refs):
    ring, (wa, wb, wc, wd), (out, normed, hidden) = refs[0:5], refs[5:9], refs[9:]
    c = index("c")
    blocks = placed(*ring)
    total = jnp.zeros((USED, 128), f32)
    for _, *halves in blocks:
        for x in halves:
            for h in range(2):
                v = x[0:USED, 128 * h : 128 * h + 128].astype(f32)
                total = total + v * v
    inverse = lax.rsqrt(jnp.sum(total, axis=1, keepdims=True) / D + epsilon)
    for y, *halves in blocks:
        for core, x in enumerate(halves):
            for h in range(2):
                lanes = slice(128 * h, 128 * h + 128)
                gain = x[USED:BLOCK, lanes].astype(f32)[0:1, :]
                column = pl.ds(pl.multiple_of(128 * slice_of(y, core, h), 128), 128)
                normed[:, column] = (x[0:USED, lanes].astype(f32) * inverse * gain).astype(bf16)
    x = normed[0:HALF, :]
    for pair, core in (((wa, wb), c), ((wc, wd), 1 - c)):
        g = dot(x, jnp.concatenate([w[0:D, :] for w in pair], axis=1))
        u = dot(x, jnp.concatenate([w[D : 2 * D, :] for w in pair], axis=1))
        out[core, 0:HALF, :] = (silu(g) * u).astype(bf16)
    packed = jnp.concatenate(
        [
            jnp.concatenate([w[PACK + 64 * b : PACK + 64 * b + 64, :] for b in range(16)], axis=1)
            for w in (wa, wc, wb, wd)
        ],
        axis=0,
    )
    s = lax.dot_general(
        normed[HALF:, :], packed, (((1,), (1,)), ((), ())), preferred_element_type=f32
    )
    h = (silu(s) * pltpu.roll(s, 256 - 32, 1)).astype(bf16)
    i = lax.broadcasted_iota(i32, (256, 128), 0)
    j = lax.broadcasted_iota(i32, (256, 128), 1)
    goes = (lax.shift_right_logical(i, 6) * 32 + (i & 31)) ^ (c * 32)
    perm = jnp.where(((i & 32) == 0) & (goes == j), 1.0, 0.0).astype(bf16)
    hidden[...] = dot(h, perm)
    for half in range(2):
        n = 48 * half
        out[half, HALF:HROWS, :] = jnp.concatenate(
            [hidden[n : n + 24, :], hidden[n + 24 : n + 48, :]], axis=1
        ).astype(bf16)


def down_body(*refs):
    ring, (wa, wb, wc, wd), (back, give, skeep, sgive, hidden) = refs[0:5], refs[5:9], refs[9:]
    blocks = placed(*ring)

    def rows_of(pair, first, count):
        n = pl.multiple_of(first, 32)
        return jnp.concatenate([w[pl.ds(n, count), :] for w in pair], axis=1)

    for pair, out, sout in (((wc, wd), give, sgive), ((wa, wb), back.at[index("c")], skeep)):
        total = jnp.zeros((HALF, 256), f32)
        shared = jnp.zeros((SHARE, 256), f32)
        for y, *halves in blocks:
            for core, x in enumerate(halves):
                w = [rows_of(pair, DOWN + 128 * slice_of(y, core, h), 128) for h in range(2)]
                total = total + dot(x[0:HALF, :], jnp.concatenate(w, axis=0))
                tail = x[HALF:HROWS, :].astype(f32)
                hidden[48 * core : 48 * core + 24, :] = tail[:, 0:128]
                hidden[48 * core + 24 : 48 * core + 48, :] = tail[:, 128:256]
            w = [
                rows_of(pair, SDOWN + 32 * slice_of(y, core, h), 32)
                for h in range(2)
                for core in range(2)
            ]
            shared = shared + dot(hidden[...].astype(bf16), jnp.concatenate(w, axis=0))
        out[...] = total.astype(bf16)
        sout[...] = shared


def combine_body(rows, cols, skeep, sother, keep, give, acc):
    yl, c = index("yl"), index("c")
    n = SP * CAP
    slot = lax.broadcasted_iota(i32, (TOK, n), 1).astype(f32)
    meta = cols[...]
    first = dot(jnp.where(slot == meta[:, 0:1], 1.0, 0.0).astype(bf16), rows[...])
    second = dot(jnp.where(slot == meta[:, 1:2], 1.0, 0.0).astype(bf16), rows[...])
    acc[...] = meta[:, 2:3] * first + meta[:, 3:4] * second
    for core, part in ((c, skeep), (1 - c, sother)):
        start = pl.multiple_of((yl * 2 + core) * SHARE, SHARE)
        acc[pl.ds(start, SHARE), :] += part[...]
    keep[...] = acc[:, 0:128]
    give[...] = acc[:, 128:256]


def final_body(aug, keep, other, out):
    out[...] = (aug[0:TOK, :].astype(f32) + keep[...] + other[...]).astype(bf16)


def sds(shape, dtype=bf16):
    return jax.ShapeDtypeStruct(shape, dtype)


def ring(block, after=None):
    up = [(i, (i + 1) % 4) for i in range(4)]
    down = [(j, i) for i, j in up]
    u = lax.ppermute(block, "yh", up)
    d = lax.ppermute(block, "yh", down)
    if after is not None:
        u, d, after = lax.optimization_barrier((u, d, after))
    u2 = lax.ppermute(u[:1], "yh", up)
    d2 = lax.ppermute(d[1:], "yh", down)
    return (block, u, d, u2, d2), after


def layer(
    outer_gate,
    inner_gate,
    conv_input,
    conv_taps,
    mix_weight,
    residual,
    norm_gain,
    routes,
    route_scores,
    expert_gate,
    expert_up,
    expert_down,
    shared_gate,
    shared_up,
    shared_down,
):
    c = index("c")
    swap = [(0, 1), (1, 0)]
    tp = ("yh", "yl", "c")

    def edge(i):
        a = lax.slice_in_dim(inner_gate, i, i + 1, axis=1).astype(f32)
        b = lax.slice_in_dim(conv_input, i, i + 1, axis=1).astype(f32)
        return (a * b).astype(bf16)

    up = [(i, i + 1) for i in range(SP - 1)]
    before = lax.ppermute(edge(TOK - 1), "sp", up)
    after = lax.ppermute(edge(0), "sp", [(j, i) for i, j in up])

    slots, cols = call(meta_body, (sds((8, TOK), f32), sds((TOK, 128), f32)), 2)(
        routes.T, route_scores.T
    )
    w_own, w_other = call(
        pick_body,
        (sds((WROWS, 128)), sds((WROWS, 128))),
        6,
        [pltpu.VMEM((D // 2, 128), bf16), pltpu.SemaphoreType.DMA((42,))],
        space=ANY,
    )(
        *(
            pltpu.with_memory_space_constraint(w, pltpu.HBM)
            for w in (expert_gate, expert_up, expert_down, shared_gate.T, shared_up.T, shared_down)
        )
    )

    mixed = call(mixer_body, sds((32, TOK)), 6)(
        outer_gate, inner_gate, conv_input, conv_taps, before, after
    )
    mixed = lax.all_gather(mixed, ("yh", "yl", "c"), axis=0, tiled=True)
    aug = call(stream_body, sds((TOK + GAIN, 128)), 4)(
        mixed, mix_weight, residual, norm_gain.reshape(1, 128)
    )
    near = lax.ppermute(aug, tp, NEAR)
    near, w_other, w_own = lax.optimization_barrier((near, w_other, w_own))
    w_got = lax.ppermute(w_other, tp, NEAR)
    w_own_c = lax.ppermute(w_own, "c", swap)
    send, shared = call(
        dispatch_body, (sds((SP * CAP, 256)), sds((2, SHARE + GAIN, 256))), 3
    )(aug, near, slots)
    arrived = lax.all_to_all(send.reshape(SP, CAP, 256), "sp", 0, 0, tiled=True)
    block = jnp.concatenate([arrived.reshape(2, HALF, 256), shared], axis=1)
    block = lax.all_to_all(block, "c", 0, 0, tiled=True)
    x_ring, w_got = ring(block, w_got)
    w_got_c = lax.ppermute(w_got, "c", swap)
    weights = (w_own, w_got, w_own_c, w_got_c)

    hidden = call(
        up_body,
        sds((2, HROWS, 256)),
        9,
        [pltpu.VMEM((USED, D), bf16), pltpu.VMEM((SHARE, 128), f32)],
        limit=16,
    )(*x_ring, *weights)
    h_ring, _ = ring(hidden)
    back, give, skeep, sgive = call(
        down_body,
        (sds((2, HALF, 256)), sds((HALF, 256)), sds((SHARE, 256), f32), sds((SHARE, 256), f32)),
        9,
        [pltpu.VMEM((SHARE, 128), f32)],
        limit=12,
    )(*h_ring, *weights)
    got = lax.ppermute(give, "c", swap)
    sgot = lax.ppermute(sgive, "c", swap)
    back = lax.dynamic_update_index_in_dim(back, got, 1 - c, 0)
    back = lax.all_to_all(back.reshape(SP, CAP, 256), "sp", 0, 0, tiled=True)
    mine, other = call(
        combine_body, (sds((TOK, 128), f32), sds((TOK, 128), f32)), 4, [pltpu.VMEM((TOK, 256), f32)]
    )(back.reshape(SP * CAP, 256), cols, skeep, sgot)
    other = lax.ppermute(other, tp, NEAR)
    return call(final_body, sds((TOK, 128)), 3)(aug, mine, other)


def solution(mesh):
    fine = Mesh(mesh.devices.reshape(SP, 4, 2, 2), ("sp", "yh", "yl", "c"))
    tp = ("yh", "yl", "c")
    in_specs = (
        P(tp, "sp"),
        P(tp, "sp"),
        P(tp, "sp"),
        P(None, tp),
        P(None, tp),
        P("sp", tp),
        P(tp),
        P("sp", None),
        P("sp", None),
        P("sp", None, tp),
        P("sp", None, tp),
        P("sp", None, tp),
        P(None, tp),
        P(None, tp),
        P(None, tp),
    )
    return jax.shard_map(
        layer, mesh=fine, in_specs=in_specs, out_specs=P("sp", tp), check_vma=False
    )
```

```python
import jax
import jax.numpy as jnp
from jax import lax
from jax.experimental import pallas as pl
from jax.experimental.pallas import tpu as pltpu
from jax.sharding import Mesh, PartitionSpec as P


epsilon = 1e-06
routed_scale = 2.5
bf16, f32, i32 = jnp.bfloat16, jnp.float32, jnp.int32

D = 2048
TOK = 384
CAP = 24
SP = 32
EXPERTS = 64
HALF = SP // 2 * CAP
SHARE = TOK // 4
GAIN = 8
MIX = 512
USED = HALF + SHARE
BLOCK = USED + GAIN
HROWS = HALF + SHARE // 4

NEAR = [(2 * y, 2 * (y ^ 1)) for y in range(8)] + [
    (2 * y + 1, 2 * ((y + (1 if y % 2 else 7)) % 8) + 1) for y in range(8)
]
DOWN = 2 * D
PACK = 3 * D
SDOWN = PACK + D // 2
WROWS = SDOWN + 512

VM = pl.BlockSpec(memory_space=pltpu.VMEM)
ANY = pl.BlockSpec(memory_space=pl.ANY)
MIB = 1 << 20


def dot(a, b):
    return lax.dot_general(a, b, (((1,), (0,)), ((), ())), preferred_element_type=f32)


def call(body, outs, count, scratch=(), limit=8, space=VM, out_space=None):
    return pl.pallas_call(
        body,
        out_shape=outs,
        in_specs=[space] * count,
        out_specs=jax.tree.map(lambda _: out_space or space, outs),
        scratch_shapes=scratch,
        compiler_params=pltpu.CompilerParams(vmem_limit_bytes=limit * MIB),
    )


def index(axis):
    return lax.axis_index(axis)


def pick_body(gate, up, down, sg, su, sd, own, other, pack, sem):
    yl = index("yl")
    copies = [
        (w.at[which], out.at[pl.ds(i * D, D)])
        for out, which in ((other, 1 - yl), (own, yl))
        for i, w in enumerate((gate, up, down))
    ] + [(sd, out.at[pl.ds(SDOWN, 512)]) for out in (other, own)]
    copies = [pltpu.make_async_copy(a, b, sem.at[i]) for i, (a, b) in enumerate(copies)]
    loads = [
        pltpu.make_async_copy(
            w.at[:, pl.ds(128 * b, 128)], pack.at[pl.ds(64 * b + 32 * i, 32)], sem.at[8 + 16 * i + b]
        )
        for i, w in enumerate((sg, su))
        for b in range(16)
    ]
    for copy in loads + copies:
        copy.start()
    for copy in loads:
        copy.wait()
    stores = [
        pltpu.make_async_copy(pack, out.at[pl.ds(PACK, D // 2)], sem.at[40 + i])
        for i, out in enumerate((own, other))
    ]
    for copy in stores:
        copy.start()
    for copy in copies + stores:
        copy.wait()


def first_body(*refs):
    outer, inner, conv, weight, residual, gain, taps, routes, scores = refs[:9]
    last, begin, product, gate, mine, taps_out, routes_out, scores_out = refs[9:17]
    a, b, g, sem = refs[17:]
    pairs = (
        (inner, a),
        (conv, b),
        (gain, g),
        (outer, gate),
        (weight, mine.at[pl.ds(0, MIX)]),
        (residual, mine.at[pl.ds(MIX, TOK)]),
        (taps, taps_out),
        (routes, routes_out),
        (scores, scores_out),
    )
    copies = [pltpu.make_async_copy(x, y, sem.at[i]) for i, (x, y) in enumerate(pairs)]
    for copy in copies:
        copy.start()
    for copy in copies[:3]:
        copy.wait()
    value = (a[...].astype(f32) * b[...].astype(f32)).astype(bf16)
    last[...] = value[:, TOK - 1 : TOK]
    begin[...] = value[:, 0:1]
    product[...] = value
    mine[MIX + TOK :, :] = jnp.broadcast_to(g[...], (GAIN, 128))
    for copy in copies[3:]:
        copy.wait()


def mixer_body(gate, value, taps, before, after, out):
    product = value[...].astype(f32)
    lane = lax.broadcasted_iota(i32, product.shape, 1)
    left = jnp.where(lane == 0, before[...].astype(f32), pltpu.roll(product, 1, 1))
    right = jnp.where(lane == TOK - 1, after[...].astype(f32), pltpu.roll(product, TOK - 1, 1))
    i = lax.broadcasted_iota(i32, (32, 32), 0)
    j = lax.broadcasted_iota(i32, (32, 32), 1)
    k = taps[...].astype(f32)
    k = [jnp.sum(jnp.where(i == j, k[n : n + 1, :], 0.0), axis=1, keepdims=True) for n in range(3)]
    filtered = k[0] * left + k[1] * product + k[2] * right
    out[...] = (gate[...].astype(f32) * filtered).astype(bf16)


def meta_body(routes, scores, rows_out, cols_out):
    yl = index("yl")
    e = lax.broadcasted_iota(i32, (EXPERTS, TOK), 0)
    m0 = e == routes[0:1, :]
    m1 = e == routes[1:2, :]
    member = jnp.where(m0 | m1, 1.0, 0.0).astype(bf16)
    a = lax.broadcasted_iota(i32, (TOK, TOK), 0)
    b = lax.broadcasted_iota(i32, (TOK, TOK), 1)
    earlier = dot(member, jnp.where(a < b, 1.0, 0.0).astype(bf16))
    base = (lax.shift_right_logical(e, 1) * CAP + 1).astype(f32)
    value = jnp.where((e & 1) == yl, base + earlier, 0.0)
    s0 = jnp.sum(jnp.where(m0, value, 0.0), axis=0, keepdims=True) - 1.0
    s1 = jnp.sum(jnp.where(m1, value, 0.0), axis=0, keepdims=True) - 1.0
    row = lax.broadcasted_iota(i32, (8, TOK), 0)
    rows_out[...] = jnp.where(row == 0, s0, s1)
    total = scores[0:1, :] + scores[1:2, :]
    w0 = scores[0:1, :] / total * routed_scale
    w1 = scores[1:2, :] / total * routed_scale
    row = lax.broadcasted_iota(i32, (128, TOK), 0)
    table = jnp.where(row == 0, s0, jnp.where(row == 1, s1, jnp.where(row == 2, w0, w1)))
    cols_out[...] = table.T


def dispatch_body(mixed, mine, near, slots, stream, send, shared, tokens):
    yl = index("yl")
    weight = jnp.concatenate([mine[0:MIX, :], near[0:MIX, :]], axis=1)
    residual = jnp.concatenate([mine[MIX : MIX + TOK, :], near[MIX : MIX + TOK, :]], axis=1)
    projected = lax.dot_general(
        mixed[...], weight, (((0,), (0,)), ((), ())), preferred_element_type=f32
    )
    tokens[...] = (residual.astype(f32) + projected).astype(bf16)
    stream[...] = tokens[:, 0:128]
    row = lax.broadcasted_iota(i32, (SP * CAP, TOK), 0).astype(f32)
    pick = (row == slots[0:1, :]) | (row == slots[1:2, :])
    send[...] = dot(jnp.where(pick, 1.0, 0.0).astype(bf16), tokens[...]).astype(bf16)
    for core in range(2):
        start = pl.multiple_of((yl * 2 + core) * SHARE, SHARE)
        shared[core, 0:SHARE, :] = tokens[pl.ds(start, SHARE), :]
        for h, x in enumerate((mine, near)):
            shared[core, SHARE : SHARE + GAIN, 128 * h : 128 * h + 128] = x[MIX + TOK :, :]


def silu(v):
    return v * (1.0 / (1.0 + jnp.exp(-v)))


def placed(own, up, down, up2, down2):
    yh, yl = index("yh"), index("yl")
    return (
        (2 * yh + yl, own.at[0], own.at[1]),
        (2 * ((yh + 3) % 4) + yl, up.at[0], up.at[1]),
        (2 * ((yh + 1) % 4) + yl, down.at[0], down.at[1]),
        (2 * ((yh + 2) % 4) + yl, up2.at[0], down2.at[0]),
    )


def slice_of(y, core, near):
    if near:
        yl = index("yl")
        y = (y + 2 * yl + 7) % 8 if core else y + 1 - 2 * yl
    return 2 * y + core


def up_body(*refs):
    ring, (wa, wb, wc, wd), (out, normed, hidden) = refs[0:5], refs[5:9], refs[9:]
    c = index("c")
    blocks = placed(*ring)
    total = jnp.zeros((USED, 128), f32)
    for _, *halves in blocks:
        for x in halves:
            for h in range(2):
                v = x[0:USED, 128 * h : 128 * h + 128].astype(f32)
                total = total + v * v
    inverse = lax.rsqrt(jnp.sum(total, axis=1, keepdims=True) / D + epsilon)
    for y, *halves in blocks:
        for core, x in enumerate(halves):
            for h in range(2):
                lanes = slice(128 * h, 128 * h + 128)
                gain = x[USED:BLOCK, lanes].astype(f32)[0:1, :]
                column = pl.ds(pl.multiple_of(128 * slice_of(y, core, h), 128), 128)
                normed[:, column] = (x[0:USED, lanes].astype(f32) * inverse * gain).astype(bf16)
    x = normed[0:HALF, :]
    for pair, core in (((wa, wb), c), ((wc, wd), 1 - c)):
        g = dot(x, jnp.concatenate([w[0:D, :] for w in pair], axis=1))
        u = dot(x, jnp.concatenate([w[D : 2 * D, :] for w in pair], axis=1))
        out[core, 0:HALF, :] = (silu(g) * u).astype(bf16)
    packed = jnp.concatenate(
        [
            jnp.concatenate([w[PACK + 64 * b : PACK + 64 * b + 64, :] for b in range(16)], axis=1)
            for w in (wa, wc, wb, wd)
        ],
        axis=0,
    )
    s = lax.dot_general(
        normed[HALF:, :], packed, (((1,), (1,)), ((), ())), preferred_element_type=f32
    )
    h = (silu(s) * pltpu.roll(s, 256 - 32, 1)).astype(bf16)
    i = lax.broadcasted_iota(i32, (256, 128), 0)
    j = lax.broadcasted_iota(i32, (256, 128), 1)
    goes = (lax.shift_right_logical(i, 6) * 32 + (i & 31)) ^ (c * 32)
    perm = jnp.where(((i & 32) == 0) & (goes == j), 1.0, 0.0).astype(bf16)
    hidden[...] = dot(h, perm)
    for half in range(2):
        n = 48 * half
        out[half, HALF:HROWS, :] = jnp.concatenate(
            [hidden[n : n + 24, :], hidden[n + 24 : n + 48, :]], axis=1
        ).astype(bf16)


def down_body(*refs):
    ring, (wa, wb, wc, wd), (back, give, skeep, sgive, hidden) = refs[0:5], refs[5:9], refs[9:]
    blocks = placed(*ring)

    def rows_of(pair, first, count):
        n = pl.multiple_of(first, 32)
        return jnp.concatenate([w[pl.ds(n, count), :] for w in pair], axis=1)

    for pair, out, sout in (((wc, wd), give, sgive), ((wa, wb), back.at[index("c")], skeep)):
        total = jnp.zeros((HALF, 256), f32)
        shared = jnp.zeros((SHARE, 256), f32)
        for y, *halves in blocks:
            for core, x in enumerate(halves):
                w = [rows_of(pair, DOWN + 128 * slice_of(y, core, h), 128) for h in range(2)]
                total = total + dot(x[0:HALF, :], jnp.concatenate(w, axis=0))
                tail = x[HALF:HROWS, :].astype(f32)
                hidden[48 * core : 48 * core + 24, :] = tail[:, 0:128]
                hidden[48 * core + 24 : 48 * core + 48, :] = tail[:, 128:256]
            w = [
                rows_of(pair, SDOWN + 32 * slice_of(y, core, h), 32)
                for h in range(2)
                for core in range(2)
            ]
            shared = shared + dot(hidden[...].astype(bf16), jnp.concatenate(w, axis=0))
        out[...] = total.astype(bf16)
        sout[...] = shared


def combine_body(rows, cols, skeep, sother, keep, give, acc):
    yl, c = index("yl"), index("c")
    n = SP * CAP
    slot = lax.broadcasted_iota(i32, (TOK, n), 1).astype(f32)
    meta = cols[...]
    first = dot(jnp.where(slot == meta[:, 0:1], 1.0, 0.0).astype(bf16), rows[...])
    second = dot(jnp.where(slot == meta[:, 1:2], 1.0, 0.0).astype(bf16), rows[...])
    acc[...] = meta[:, 2:3] * first + meta[:, 3:4] * second
    for core, part in ((c, skeep), (1 - c, sother)):
        start = pl.multiple_of((yl * 2 + core) * SHARE, SHARE)
        acc[pl.ds(start, SHARE), :] += part[...]
    keep[...] = acc[:, 0:128]
    give[...] = acc[:, 128:256]


def final_body(stream, keep, other, out):
    out[...] = (stream[...].astype(f32) + keep[...] + other[...]).astype(bf16)


def sds(shape, dtype=bf16):
    return jax.ShapeDtypeStruct(shape, dtype)


def ring(block, after=None):
    up = [(i, (i + 1) % 4) for i in range(4)]
    down = [(j, i) for i, j in up]
    u = lax.ppermute(block, "yh", up)
    d = lax.ppermute(block, "yh", down)
    if after is not None:
        u, d, after = lax.optimization_barrier((u, d, after))
    u2 = lax.ppermute(u[:1], "yh", up)
    d2 = lax.ppermute(d[1:], "yh", down)
    return (block, u, d, u2, d2), after


def layer(
    outer_gate,
    inner_gate,
    conv_input,
    conv_taps,
    mix_weight,
    residual,
    norm_gain,
    routes,
    route_scores,
    expert_gate,
    expert_up,
    expert_down,
    shared_gate,
    shared_up,
    shared_down,
):
    c = index("c")
    swap = [(0, 1), (1, 0)]
    tp = ("yh", "yl", "c")

    column = sds((32, 1))
    last, begin, product, gate, mine, taps, chosen, scores = call(
        first_body,
        (
            column,
            column,
            sds((32, TOK)),
            sds((32, TOK)),
            sds((MIX + TOK + GAIN, 128)),
            sds((3, 32)),
            sds((2, TOK), i32),
            sds((2, TOK), f32),
        ),
        9,
        [
            pltpu.VMEM((32, TOK), bf16),
            pltpu.VMEM((32, TOK), bf16),
            pltpu.VMEM((1, 128), bf16),
            pltpu.SemaphoreType.DMA((9,)),
        ],
        space=ANY,
        out_space=VM,
    )(
        *(
            pltpu.with_memory_space_constraint(w, pltpu.HBM)
            for w in (
                outer_gate,
                inner_gate,
                conv_input,
                mix_weight,
                residual,
                norm_gain.reshape(1, 128),
                conv_taps,
                routes.T,
                route_scores.T,
            )
        )
    )
    up = [(i, i + 1) for i in range(SP - 1)]
    before = lax.ppermute(last, "sp", up)
    after = lax.ppermute(begin, "sp", [(j, i) for i, j in up])
    near = lax.ppermute(mine, tp, NEAR)

    slots, cols = call(meta_body, (sds((8, TOK), f32), sds((TOK, 128), f32)), 2)(chosen, scores)
    w_own, w_other = call(
        pick_body,
        (sds((WROWS, 128)), sds((WROWS, 128))),
        6,
        [pltpu.VMEM((D // 2, 128), bf16), pltpu.SemaphoreType.DMA((42,))],
        space=ANY,
    )(
        *(
            pltpu.with_memory_space_constraint(w, pltpu.HBM)
            for w in (expert_gate, expert_up, expert_down, shared_gate.T, shared_up.T, shared_down)
        )
    )

    mixed = call(mixer_body, sds((32, TOK)), 5)(
        gate, product, taps, before, after
    )
    mixed, near, w_other, w_own = lax.optimization_barrier((mixed, near, w_other, w_own))
    mixed = lax.all_gather(mixed, tp, axis=0, tiled=True)
    mixed, w_other, w_own = lax.optimization_barrier((mixed, w_other, w_own))
    w_got = lax.ppermute(w_other, tp, NEAR)
    w_own_c = lax.ppermute(w_own, "c", swap)
    stream, send, shared = call(
        dispatch_body,
        (sds((TOK, 128)), sds((SP * CAP, 256)), sds((2, SHARE + GAIN, 256))),
        4,
        [pltpu.VMEM((TOK, 256), bf16)],
    )(mixed, mine, near, slots)
    arrived = lax.all_to_all(send.reshape(SP, CAP, 256), "sp", 0, 0, tiled=True)
    block = jnp.concatenate([arrived.reshape(2, HALF, 256), shared], axis=1)
    block = lax.all_to_all(block, "c", 0, 0, tiled=True)
    x_ring, w_got = ring(block, w_got)
    w_got_c = lax.ppermute(w_got, "c", swap)
    weights = (w_own, w_got, w_own_c, w_got_c)

    hidden = call(
        up_body,
        sds((2, HROWS, 256)),
        9,
        [pltpu.VMEM((USED, D), bf16), pltpu.VMEM((SHARE, 128), f32)],
        limit=16,
    )(*x_ring, *weights)
    h_ring, _ = ring(hidden)
    back, give, skeep, sgive = call(
        down_body,
        (sds((2, HALF, 256)), sds((HALF, 256)), sds((SHARE, 256), f32), sds((SHARE, 256), f32)),
        9,
        [pltpu.VMEM((SHARE, 128), f32)],
        limit=12,
    )(*h_ring, *weights)
    got = lax.ppermute(give, "c", swap)
    sgot = lax.ppermute(sgive, "c", swap)
    back = lax.dynamic_update_index_in_dim(back, got, 1 - c, 0)
    back = lax.all_to_all(back.reshape(SP, CAP, 256), "sp", 0, 0, tiled=True)
    keep, other = call(
        combine_body, (sds((TOK, 128), f32), sds((TOK, 128), f32)), 4, [pltpu.VMEM((TOK, 256), f32)]
    )(back.reshape(SP * CAP, 256), cols, skeep, sgot)
    other = lax.ppermute(other, tp, NEAR)
    return call(final_body, sds((TOK, 128)), 3)(stream, keep, other)


def solution(mesh):
    fine = Mesh(mesh.devices.reshape(SP, 4, 2, 2), ("sp", "yh", "yl", "c"))
    tp = ("yh", "yl", "c")
    in_specs = (
        P(tp, "sp"),
        P(tp, "sp"),
        P(tp, "sp"),
        P(None, tp),
        P(None, tp),
        P("sp", tp),
        P(tp),
        P("sp", None),
        P("sp", None),
        P("sp", None, tp),
        P("sp", None, tp),
        P("sp", None, tp),
        P(None, tp),
        P(None, tp),
        P(None, tp),
    )
    return jax.shard_map(
        layer, mesh=fine, in_specs=in_specs, out_specs=P("sp", tp), check_vma=False
    )
```

```python
import functools

import jax
import jax.numpy as jnp
from jax import lax
from jax.experimental import pallas as pl
from jax.experimental.pallas import tpu as pltpu
from jax.sharding import Mesh, PartitionSpec as P


epsilon = 1e-06
routed_scale = 2.5
bf16, f32, i32 = jnp.bfloat16, jnp.float32, jnp.int32

D = 2048
TOK = 384
CAP = 24
SP = 32
EXPERTS = 64
HALF = SP // 2 * CAP
SHARE = TOK // 4
GAIN = 8
MIX = 512
USED = HALF + SHARE
BLOCK = USED + GAIN
HROWS = HALF + SHARE // 4

NEAR = [(2 * y, 2 * (y ^ 1)) for y in range(8)] + [
    (2 * y + 1, 2 * ((y + (1 if y % 2 else 7)) % 8) + 1) for y in range(8)
]
DOWN = 2 * D
PACK = 3 * D
SDOWN = PACK + D // 2
WROWS = SDOWN + 512

VM = pl.BlockSpec(memory_space=pltpu.VMEM)
ANY = pl.BlockSpec(memory_space=pl.ANY)
MIB = 1 << 20


def dot(a, b):
    return lax.dot_general(a, b, (((1,), (0,)), ((), ())), preferred_element_type=f32)


def call(body, outs, count, scratch=(), limit=8, space=VM, out_space=None):
    return pl.pallas_call(
        body,
        out_shape=outs,
        in_specs=[space] * count,
        out_specs=jax.tree.map(lambda _: out_space or space, outs),
        scratch_shapes=scratch,
        compiler_params=pltpu.CompilerParams(vmem_limit_bytes=limit * MIB),
    )


def index(axis):
    return lax.axis_index(axis)


def pick_body(mine, gate, up, down, sg, su, sd, out, pack, sem):
    which = index("yl") if mine else 1 - index("yl")
    copies = [(w.at[which], out.at[pl.ds(i * D, D)]) for i, w in enumerate((gate, up, down))]
    copies.append((sd, out.at[pl.ds(SDOWN, 512)]))
    copies = [pltpu.make_async_copy(a, b, sem.at[i]) for i, (a, b) in enumerate(copies)]
    loads = [
        pltpu.make_async_copy(
            w.at[:, pl.ds(128 * b, 128)], pack.at[pl.ds(64 * b + 32 * i, 32)], sem.at[4 + 16 * i + b]
        )
        for i, w in enumerate((sg, su))
        for b in range(16)
    ]
    for copy in loads + copies:
        copy.start()
    for copy in loads:
        copy.wait()
    store = pltpu.make_async_copy(pack, out.at[pl.ds(PACK, D // 2)], sem.at[36])
    store.start()
    for copy in copies + [store]:
        copy.wait()


def first_body(*refs):
    outer, inner, conv, weight, residual, gain, taps, routes, scores = refs[:9]
    last, begin, product, gate, mine, taps_out, routes_out, scores_out = refs[9:17]
    a, b, g, sem = refs[17:]
    pairs = (
        (inner, a),
        (conv, b),
        (gain, g),
        (outer, gate),
        (weight, mine.at[pl.ds(0, MIX)]),
        (residual, mine.at[pl.ds(MIX, TOK)]),
        (taps, taps_out),
        (routes, routes_out),
        (scores, scores_out),
    )
    copies = [pltpu.make_async_copy(x, y, sem.at[i]) for i, (x, y) in enumerate(pairs)]
    for copy in copies:
        copy.start()
    for copy in copies[:3]:
        copy.wait()
    value = (a[...].astype(f32) * b[...].astype(f32)).astype(bf16)
    last[...] = value[:, TOK - 1 : TOK]
    begin[...] = value[:, 0:1]
    product[...] = value
    mine[MIX + TOK :, :] = jnp.broadcast_to(g[...], (GAIN, 128))
    for copy in copies[3:]:
        copy.wait()


def mixer_body(gate, value, taps, before, after, out):
    product = value[...].astype(f32)
    lane = lax.broadcasted_iota(i32, product.shape, 1)
    left = jnp.where(lane == 0, before[...].astype(f32), pltpu.roll(product, 1, 1))
    right = jnp.where(lane == TOK - 1, after[...].astype(f32), pltpu.roll(product, TOK - 1, 1))
    i = lax.broadcasted_iota(i32, (32, 32), 0)
    j = lax.broadcasted_iota(i32, (32, 32), 1)
    k = taps[...].astype(f32)
    k = [jnp.sum(jnp.where(i == j, k[n : n + 1, :], 0.0), axis=1, keepdims=True) for n in range(3)]
    filtered = k[0] * left + k[1] * product + k[2] * right
    out[...] = (gate[...].astype(f32) * filtered).astype(bf16)


def meta_body(routes, scores, rows_out, cols_out):
    yl = index("yl")
    e = lax.broadcasted_iota(i32, (EXPERTS, TOK), 0)
    m0 = e == routes[0:1, :]
    m1 = e == routes[1:2, :]
    member = jnp.where(m0 | m1, 1.0, 0.0).astype(bf16)
    a = lax.broadcasted_iota(i32, (TOK, TOK), 0)
    b = lax.broadcasted_iota(i32, (TOK, TOK), 1)
    earlier = dot(member, jnp.where(a < b, 1.0, 0.0).astype(bf16))
    base = (lax.shift_right_logical(e, 1) * CAP + 1).astype(f32)
    value = jnp.where((e & 1) == yl, base + earlier, 0.0)
    s0 = jnp.sum(jnp.where(m0, value, 0.0), axis=0, keepdims=True) - 1.0
    s1 = jnp.sum(jnp.where(m1, value, 0.0), axis=0, keepdims=True) - 1.0
    row = lax.broadcasted_iota(i32, (8, TOK), 0)
    rows_out[...] = jnp.where(row == 0, s0, s1)
    total = scores[0:1, :] + scores[1:2, :]
    w0 = scores[0:1, :] / total * routed_scale
    w1 = scores[1:2, :] / total * routed_scale
    row = lax.broadcasted_iota(i32, (128, TOK), 0)
    table = jnp.where(row == 0, s0, jnp.where(row == 1, s1, jnp.where(row == 2, w0, w1)))
    cols_out[...] = table.T


def dispatch_body(mixed, mine, near, slots, stream, send, shared, tokens):
    yl = index("yl")
    weight = jnp.concatenate([mine[0:MIX, :], near[0:MIX, :]], axis=1)
    residual = jnp.concatenate([mine[MIX : MIX + TOK, :], near[MIX : MIX + TOK, :]], axis=1)
    projected = lax.dot_general(
        mixed[...], weight, (((0,), (0,)), ((), ())), preferred_element_type=f32
    )
    tokens[...] = (residual.astype(f32) + projected).astype(bf16)
    stream[...] = tokens[:, 0:128]
    row = lax.broadcasted_iota(i32, (SP * CAP, TOK), 0).astype(f32)
    pick = (row == slots[0:1, :]) | (row == slots[1:2, :])
    send[...] = dot(jnp.where(pick, 1.0, 0.0).astype(bf16), tokens[...]).astype(bf16)
    for core in range(2):
        start = pl.multiple_of((yl * 2 + core) * SHARE, SHARE)
        shared[core, 0:SHARE, :] = tokens[pl.ds(start, SHARE), :]
        for h, x in enumerate((mine, near)):
            shared[core, SHARE : SHARE + GAIN, 128 * h : 128 * h + 128] = x[MIX + TOK :, :]


def silu(v):
    return v * (1.0 / (1.0 + jnp.exp(-v)))


def placed(own, up_low, up_high, down_low, down_high, far_low, far_high):
    yh, yl = index("yh"), index("yl")
    return (
        (2 * yh + yl, own.at[0], own.at[1]),
        (2 * ((yh + 3) % 4) + yl, up_low, up_high),
        (2 * ((yh + 1) % 4) + yl, down_low, down_high),
        (2 * ((yh + 2) % 4) + yl, far_low, far_high),
    )


def slice_of(y, core, near):
    if near:
        yl = index("yl")
        y = (y + 2 * yl + 7) % 8 if core else y + 1 - 2 * yl
    return 2 * y + core


def up_body(*refs):
    ring, (wa, wb, wc, wd), (out, normed, hidden) = refs[0:7], refs[7:11], refs[11:]
    c = index("c")
    blocks = placed(*ring)
    total = jnp.zeros((USED, 128), f32)
    for _, *halves in blocks:
        for x in halves:
            for h in range(2):
                v = x[0:USED, 128 * h : 128 * h + 128].astype(f32)
                total = total + v * v
    inverse = lax.rsqrt(jnp.sum(total, axis=1, keepdims=True) / D + epsilon)
    for y, *halves in blocks:
        for core, x in enumerate(halves):
            for h in range(2):
                lanes = slice(128 * h, 128 * h + 128)
                gain = x[USED:BLOCK, lanes].astype(f32)[0:1, :]
                column = pl.ds(pl.multiple_of(128 * slice_of(y, core, h), 128), 128)
                normed[:, column] = (x[0:USED, lanes].astype(f32) * inverse * gain).astype(bf16)
    x = normed[0:HALF, :]
    for pair, core in (((wa, wb), c), ((wc, wd), 1 - c)):
        g = dot(x, jnp.concatenate([w[0:D, :] for w in pair], axis=1))
        u = dot(x, jnp.concatenate([w[D : 2 * D, :] for w in pair], axis=1))
        out[core, 0:HALF, :] = (silu(g) * u).astype(bf16)
    packed = jnp.concatenate(
        [
            jnp.concatenate([w[PACK + 64 * b : PACK + 64 * b + 64, :] for b in range(16)], axis=1)
            for w in (wa, wc, wb, wd)
        ],
        axis=0,
    )
    s = lax.dot_general(
        normed[HALF:, :], packed, (((1,), (1,)), ((), ())), preferred_element_type=f32
    )
    h = (silu(s) * pltpu.roll(s, 256 - 32, 1)).astype(bf16)
    i = lax.broadcasted_iota(i32, (256, 128), 0)
    j = lax.broadcasted_iota(i32, (256, 128), 1)
    goes = (lax.shift_right_logical(i, 6) * 32 + (i & 31)) ^ (c * 32)
    perm = jnp.where(((i & 32) == 0) & (goes == j), 1.0, 0.0).astype(bf16)
    hidden[...] = dot(h, perm)
    for half in range(2):
        n = 48 * half
        out[half, HALF:HROWS, :] = jnp.concatenate(
            [hidden[n : n + 24, :], hidden[n + 24 : n + 48, :]], axis=1
        ).astype(bf16)


def down_body(*refs):
    ring, (wa, wb, wc, wd), (back, give, skeep, sgive, hidden) = refs[0:7], refs[7:11], refs[11:]
    blocks = placed(*ring)

    def rows_of(pair, first, count):
        n = pl.multiple_of(first, 32)
        return jnp.concatenate([w[pl.ds(n, count), :] for w in pair], axis=1)

    for pair, out, sout in (((wc, wd), give, sgive), ((wa, wb), back.at[index("c")], skeep)):
        total = jnp.zeros((HALF, 256), f32)
        shared = jnp.zeros((SHARE, 256), f32)
        for y, *halves in blocks:
            for core, x in enumerate(halves):
                w = [rows_of(pair, DOWN + 128 * slice_of(y, core, h), 128) for h in range(2)]
                total = total + dot(x[0:HALF, :], jnp.concatenate(w, axis=0))
                tail = x[HALF:HROWS, :].astype(f32)
                hidden[48 * core : 48 * core + 24, :] = tail[:, 0:128]
                hidden[48 * core + 24 : 48 * core + 48, :] = tail[:, 128:256]
            w = [
                rows_of(pair, SDOWN + 32 * slice_of(y, core, h), 32)
                for h in range(2)
                for core in range(2)
            ]
            shared = shared + dot(hidden[...].astype(bf16), jnp.concatenate(w, axis=0))
        out[...] = total.astype(bf16)
        sout[...] = shared


def combine_body(rows, cols, skeep, sother, keep, give, acc):
    yl, c = index("yl"), index("c")
    n = SP * CAP
    slot = lax.broadcasted_iota(i32, (TOK, n), 1).astype(f32)
    meta = cols[...]
    first = dot(jnp.where(slot == meta[:, 0:1], 1.0, 0.0).astype(bf16), rows[...])
    second = dot(jnp.where(slot == meta[:, 1:2], 1.0, 0.0).astype(bf16), rows[...])
    acc[...] = meta[:, 2:3] * first + meta[:, 3:4] * second
    for core, part in ((c, skeep), (1 - c, sother)):
        start = pl.multiple_of((yl * 2 + core) * SHARE, SHARE)
        acc[pl.ds(start, SHARE), :] += part[...]
    keep[...] = acc[:, 0:128]
    give[...] = acc[:, 128:256]


def final_body(stream, keep, other, out):
    out[...] = (stream[...].astype(f32) + keep[...] + other[...]).astype(bf16)


def sds(shape, dtype=bf16):
    return jax.ShapeDtypeStruct(shape, dtype)


def ring(block):
    up = [(i, (i + 1) % 4) for i in range(4)]
    down = [(j, i) for i, j in up]
    low, high = block[0], block[1]
    up_low = lax.ppermute(low, "yh", up)
    down_high = lax.ppermute(high, "yh", down)
    up_high = lax.ppermute(high, "yh", up)
    down_low = lax.ppermute(low, "yh", down)
    far_low = lax.ppermute(up_low, "yh", up)
    far_high = lax.ppermute(down_high, "yh", down)
    return (block, up_low, up_high, down_low, down_high, far_low, far_high)


def layer(
    outer_gate,
    inner_gate,
    conv_input,
    conv_taps,
    mix_weight,
    residual,
    norm_gain,
    routes,
    route_scores,
    expert_gate,
    expert_up,
    expert_down,
    shared_gate,
    shared_up,
    shared_down,
):
    c = index("c")
    swap = [(0, 1), (1, 0)]
    tp = ("yh", "yl", "c")

    column = sds((32, 1))
    last, begin, product, gate, mine, taps, chosen, scores = call(
        first_body,
        (
            column,
            column,
            sds((32, TOK)),
            sds((32, TOK)),
            sds((MIX + TOK + GAIN, 128)),
            sds((3, 32)),
            sds((2, TOK), i32),
            sds((2, TOK), f32),
        ),
        9,
        [
            pltpu.VMEM((32, TOK), bf16),
            pltpu.VMEM((32, TOK), bf16),
            pltpu.VMEM((1, 128), bf16),
            pltpu.SemaphoreType.DMA((9,)),
        ],
        space=ANY,
        out_space=VM,
    )(
        *(
            pltpu.with_memory_space_constraint(w, pltpu.HBM)
            for w in (
                outer_gate,
                inner_gate,
                conv_input,
                mix_weight,
                residual,
                norm_gain.reshape(1, 128),
                conv_taps,
                routes.T,
                route_scores.T,
            )
        )
    )
    up = [(i, i + 1) for i in range(SP - 1)]
    before = lax.ppermute(last, "sp", up)
    after = lax.ppermute(begin, "sp", [(j, i) for i, j in up])
    near = lax.ppermute(mine, tp, NEAR)

    slots, cols = call(meta_body, (sds((8, TOK), f32), sds((TOK, 128), f32)), 2)(chosen, scores)

    def picked(mine):
        return call(
            functools.partial(pick_body, mine),
            sds((WROWS, 128)),
            6,
            [pltpu.VMEM((D // 2, 128), bf16), pltpu.SemaphoreType.DMA((37,))],
            space=ANY,
        )(
            *(
                pltpu.with_memory_space_constraint(w, pltpu.HBM)
                for w in (expert_gate, expert_up, expert_down, shared_gate.T, shared_up.T, shared_down)
            )
        )

    w_other = picked(False)
    w_own = picked(True)

    mixed = call(mixer_body, sds((32, TOK)), 5)(
        gate, product, taps, before, after
    )
    mixed, near, w_other = lax.optimization_barrier((mixed, near, w_other))
    mixed = lax.all_gather(mixed, tp, axis=0, tiled=True)
    mixed, w_other = lax.optimization_barrier((mixed, w_other))
    w_got = lax.ppermute(w_other, tp, NEAR)
    w_own_c = lax.ppermute(w_own, "c", swap)
    stream, send, shared = call(
        dispatch_body,
        (sds((TOK, 128)), sds((SP * CAP, 256)), sds((2, SHARE + GAIN, 256))),
        4,
        [pltpu.VMEM((TOK, 256), bf16)],
    )(mixed, mine, near, slots)
    arrived = lax.all_to_all(send.reshape(SP, CAP, 256), "sp", 0, 0, tiled=True)
    block = jnp.concatenate([arrived.reshape(2, HALF, 256), shared], axis=1)
    block = lax.all_to_all(block, "c", 0, 0, tiled=True)
    x_ring = ring(block)
    w_got_c = lax.ppermute(w_got, "c", swap)
    weights = (w_own, w_got, w_own_c, w_got_c)

    hidden = call(
        up_body,
        sds((2, HROWS, 256)),
        11,
        [pltpu.VMEM((USED, D), bf16), pltpu.VMEM((SHARE, 128), f32)],
        limit=16,
    )(*x_ring, *weights)
    h_ring = ring(hidden)
    back, give, skeep, sgive = call(
        down_body,
        (sds((2, HALF, 256)), sds((HALF, 256)), sds((SHARE, 256), f32), sds((SHARE, 256), f32)),
        11,
        [pltpu.VMEM((SHARE, 128), f32)],
        limit=12,
    )(*h_ring, *weights)
    got = lax.ppermute(give, "c", swap)
    sgot = lax.ppermute(sgive, "c", swap)
    back = lax.dynamic_update_index_in_dim(back, got, 1 - c, 0)
    back = lax.all_to_all(back.reshape(SP, CAP, 256), "sp", 0, 0, tiled=True)
    keep, other = call(
        combine_body, (sds((TOK, 128), f32), sds((TOK, 128), f32)), 4, [pltpu.VMEM((TOK, 256), f32)]
    )(back.reshape(SP * CAP, 256), cols, skeep, sgot)
    other = lax.ppermute(other, tp, NEAR)
    return call(final_body, sds((TOK, 128)), 3)(stream, keep, other)


def solution(mesh):
    fine = Mesh(mesh.devices.reshape(SP, 4, 2, 2), ("sp", "yh", "yl", "c"))
    tp = ("yh", "yl", "c")
    in_specs = (
        P(tp, "sp"),
        P(tp, "sp"),
        P(tp, "sp"),
        P(None, tp),
        P(None, tp),
        P("sp", tp),
        P(tp),
        P("sp", None),
        P("sp", None),
        P("sp", None, tp),
        P("sp", None, tp),
        P("sp", None, tp),
        P(None, tp),
        P(None, tp),
        P(None, tp),
    )
    return jax.shard_map(
        layer, mesh=fine, in_specs=in_specs, out_specs=P("sp", tp), check_vma=False
    )
```

```python
import functools

import jax
import jax.numpy as jnp
from jax import lax
from jax.experimental import pallas as pl
from jax.experimental.pallas import tpu as pltpu
from jax.sharding import Mesh, PartitionSpec as P


epsilon = 1e-06
routed_scale = 2.5
bf16, f32, i32 = jnp.bfloat16, jnp.float32, jnp.int32

D = 2048
TOK = 384
CAP = 24
SP = 32
EXPERTS = 64
HALF = SP // 2 * CAP
SHARE = TOK // 4
GAIN = 8
MIX = 512
USED = HALF + SHARE
BLOCK = USED + GAIN
HROWS = HALF + SHARE // 4

NEAR = [(2 * y, 2 * (y ^ 1)) for y in range(8)] + [
    (2 * y + 1, 2 * ((y + (1 if y % 2 else 7)) % 8) + 1) for y in range(8)
]
DOWN = 2 * D
PACK = 3 * D
SDOWN = PACK + D // 2
WROWS = SDOWN + 512

VM = pl.BlockSpec(memory_space=pltpu.VMEM)
ANY = pl.BlockSpec(memory_space=pl.ANY)
MIB = 1 << 20


def dot(a, b):
    return lax.dot_general(a, b, (((1,), (0,)), ((), ())), preferred_element_type=f32)


def call(body, outs, count, scratch=(), limit=8, space=VM, out_space=None):
    return pl.pallas_call(
        body,
        out_shape=outs,
        in_specs=[space] * count,
        out_specs=jax.tree.map(lambda _: out_space or space, outs),
        scratch_shapes=scratch,
        compiler_params=pltpu.CompilerParams(vmem_limit_bytes=limit * MIB),
    )


def index(axis):
    return lax.axis_index(axis)


def pick_body(mine, gate, up, down, sg, su, sd, out, pack, sem):
    which = index("yl") if mine else 1 - index("yl")
    copies = [(w.at[which], out.at[pl.ds(i * D, D)]) for i, w in enumerate((gate, up, down))]
    copies.append((sd, out.at[pl.ds(SDOWN, 512)]))
    copies = [pltpu.make_async_copy(a, b, sem.at[i]) for i, (a, b) in enumerate(copies)]
    loads = [
        pltpu.make_async_copy(
            w.at[:, pl.ds(128 * b, 128)], pack.at[pl.ds(64 * b + 32 * i, 32)], sem.at[4 + 16 * i + b]
        )
        for i, w in enumerate((sg, su))
        for b in range(16)
    ]
    for copy in loads + copies:
        copy.start()
    for copy in loads:
        copy.wait()
    store = pltpu.make_async_copy(pack, out.at[pl.ds(PACK, D // 2)], sem.at[36])
    store.start()
    for copy in copies + [store]:
        copy.wait()


def first_body(*refs):
    outer, inner, conv, weight, residual, gain, taps, routes, scores = refs[:9]
    last, begin, product, gate, mine, taps_out, routes_out, scores_out = refs[9:17]
    a, b, g, sem = refs[17:]
    pairs = (
        (inner, a),
        (conv, b),
        (gain, g),
        (outer, gate),
        (weight, mine.at[pl.ds(0, MIX)]),
        (residual, mine.at[pl.ds(MIX, TOK)]),
        (taps, taps_out),
        (routes, routes_out),
        (scores, scores_out),
    )
    copies = [pltpu.make_async_copy(x, y, sem.at[i]) for i, (x, y) in enumerate(pairs)]
    for copy in copies:
        copy.start()
    for copy in copies[:3]:
        copy.wait()
    value = (a[...].astype(f32) * b[...].astype(f32)).astype(bf16)
    last[...] = value[:, TOK - 1 : TOK]
    begin[...] = value[:, 0:1]
    product[...] = value
    mine[MIX + TOK :, :] = jnp.broadcast_to(g[...], (GAIN, 128))
    for copy in copies[3:]:
        copy.wait()


def mixer_body(gate, value, taps, before, after, out):
    product = value[...].astype(f32)
    lane = lax.broadcasted_iota(i32, product.shape, 1)
    left = jnp.where(lane == 0, before[...].astype(f32), pltpu.roll(product, 1, 1))
    right = jnp.where(lane == TOK - 1, after[...].astype(f32), pltpu.roll(product, TOK - 1, 1))
    i = lax.broadcasted_iota(i32, (32, 32), 0)
    j = lax.broadcasted_iota(i32, (32, 32), 1)
    k = taps[...].astype(f32)
    k = [jnp.sum(jnp.where(i == j, k[n : n + 1, :], 0.0), axis=1, keepdims=True) for n in range(3)]
    filtered = k[0] * left + k[1] * product + k[2] * right
    out[...] = (gate[...].astype(f32) * filtered).astype(bf16)


def meta_body(routes, scores, rows_out, cols_out):
    yl = index("yl")
    e = lax.broadcasted_iota(i32, (EXPERTS, TOK), 0)
    m0 = e == routes[0:1, :]
    m1 = e == routes[1:2, :]
    member = jnp.where(m0 | m1, 1.0, 0.0).astype(bf16)
    a = lax.broadcasted_iota(i32, (TOK, TOK), 0)
    b = lax.broadcasted_iota(i32, (TOK, TOK), 1)
    earlier = dot(member, jnp.where(a < b, 1.0, 0.0).astype(bf16))
    base = (lax.shift_right_logical(e, 1) * CAP + 1).astype(f32)
    value = jnp.where((e & 1) == yl, base + earlier, 0.0)
    s0 = jnp.sum(jnp.where(m0, value, 0.0), axis=0, keepdims=True) - 1.0
    s1 = jnp.sum(jnp.where(m1, value, 0.0), axis=0, keepdims=True) - 1.0
    row = lax.broadcasted_iota(i32, (8, TOK), 0)
    rows_out[...] = jnp.where(row == 0, s0, s1)
    total = scores[0:1, :] + scores[1:2, :]
    w0 = scores[0:1, :] / total * routed_scale
    w1 = scores[1:2, :] / total * routed_scale
    row = lax.broadcasted_iota(i32, (128, TOK), 0)
    table = jnp.where(row == 0, s0, jnp.where(row == 1, s1, jnp.where(row == 2, w0, w1)))
    cols_out[...] = table.T


def dispatch_body(mixed, mine, near, slots, stream, send, shared, tokens):
    yl = index("yl")
    weight = jnp.concatenate([mine[0:MIX, :], near[0:MIX, :]], axis=1)
    residual = jnp.concatenate([mine[MIX : MIX + TOK, :], near[MIX : MIX + TOK, :]], axis=1)
    projected = lax.dot_general(
        mixed[...], weight, (((0,), (0,)), ((), ())), preferred_element_type=f32
    )
    tokens[...] = (residual.astype(f32) + projected).astype(bf16)
    stream[...] = tokens[:, 0:128]
    row = lax.broadcasted_iota(i32, (SP * CAP, TOK), 0).astype(f32)
    pick = (row == slots[0:1, :]) | (row == slots[1:2, :])
    send[...] = dot(jnp.where(pick, 1.0, 0.0).astype(bf16), tokens[...]).astype(bf16)
    for core in range(2):
        start = pl.multiple_of((yl * 2 + core) * SHARE, SHARE)
        shared[core, 0:SHARE, :] = tokens[pl.ds(start, SHARE), :]
        for h, x in enumerate((mine, near)):
            shared[core, SHARE : SHARE + GAIN, 128 * h : 128 * h + 128] = x[MIX + TOK :, :]


def silu(v):
    return v * (1.0 / (1.0 + jnp.exp(-v)))


def split_body(arrived, shared, mine, give):
    c = index("c")
    for out, core in ((mine, c), (give, 1 - c)):
        out[0:HALF, :] = arrived[pl.ds(pl.multiple_of(core * HALF, HALF), HALF), :]
        out[HALF:, :] = shared[core]


def placed(mine, other, up_mine, up_other, down_mine, down_other, far_mine, far_other):
    yh, yl = index("yh"), index("yl")
    return (
        (2 * yh + yl, mine, other),
        (2 * ((yh + 3) % 4) + yl, up_mine, up_other),
        (2 * ((yh + 1) % 4) + yl, down_mine, down_other),
        (2 * ((yh + 2) % 4) + yl, far_mine, far_other),
    )


def slice_of(y, core, near):
    if near:
        yl = index("yl")
        y = jnp.where(core == 1, (y + 2 * yl + 7) % 8, y + 1 - 2 * yl)
    return 2 * y + core


def rows_of(weights, first, count):
    n = pl.multiple_of(first, 32)
    return jnp.concatenate([w[pl.ds(n, count), :] for w in weights], axis=1)


def pieces(y, c):
    return [slice_of(y, core, h) for core in (c, 1 - c) for h in range(2)]


def up_part(blocks, weights, scaled, squares):
    wa, wb, wc, wd = weights
    c = index("c")
    for n, (y, *halves) in enumerate(blocks):
        for i, x in enumerate(halves):
            for h in range(2):
                lanes = slice(128 * h, 128 * h + 128)
                v = x[0:USED, lanes].astype(f32)
                squares = squares + v * v
                gain = x[USED:BLOCK, lanes].astype(f32)[0:1, :]
                at = 512 * n + 256 * i + 128 * h
                scaled[:, at : at + 128] = (v * gain).astype(bf16)
    results = []
    for pair in ((wa, wb), (wc, wd)):
        for base in (0, D):
            total = jnp.zeros((HALF, 256), f32)
            for n, (y, *_) in enumerate(blocks):
                w = [rows_of(pair, base + 128 * p, 128) for p in pieces(y, c)]
                x = scaled[0:HALF, 512 * n : 512 * n + 512]
                total = total + dot(x, jnp.concatenate(w, axis=0))
            results.append(total)
    shared = jnp.zeros((SHARE, 256), f32)
    for n, (y, *_) in enumerate(blocks):
        packed = jnp.concatenate(
            [
                jnp.concatenate([rows_of([w], PACK + 64 * p, 64) for p in pieces(y, c)], axis=1)
                for w in (wa, wc, wb, wd)
            ],
            axis=0,
        )
        x = scaled[HALF:USED, 512 * n : 512 * n + 512]
        shared = shared + lax.dot_general(
            x, packed, (((1,), (1,)), ((), ())), preferred_element_type=f32
        )
    return squares, results, shared


def up_near_body(*refs):
    halves, weights, (squares, products, shared, scaled) = refs[0:6], refs[6:10], refs[10:]
    blocks = placed(*halves, None, None)[:3]
    total, results, part = up_part(blocks, weights, scaled, jnp.zeros((USED, 128), f32))
    squares[...] = total
    for i, value in enumerate(results):
        products[i] = value
    shared[...] = part


def up_far_body(*refs):
    far, weights, (squares, products, shared), (mine, other, scaled, hidden) = (
        refs[0:2],
        refs[2:6],
        refs[6:9],
        refs[9:],
    )
    c = index("c")
    blocks = placed(*[None] * 6, *far)[3:]
    total, results, part = up_part(blocks, weights, scaled, squares[...])
    inverse = lax.rsqrt(jnp.sum(total, axis=1, keepdims=True) / D + epsilon)
    rows = inverse[0:HALF]
    for i, out in enumerate((mine, other)):
        g = (products[2 * i] + results[2 * i]) * rows
        u = (products[2 * i + 1] + results[2 * i + 1]) * rows
        out[0:HALF, :] = (silu(g) * u).astype(bf16)
    s = (shared[...] + part) * inverse[HALF:]
    h = (silu(s) * pltpu.roll(s, 256 - 32, 1)).astype(bf16)
    i = lax.broadcasted_iota(i32, (256, 128), 0)
    j = lax.broadcasted_iota(i32, (256, 128), 1)
    goes = (lax.shift_right_logical(i, 6) * 32 + (i & 31)) ^ (c * 32)
    perm = jnp.where(((i & 32) == 0) & (goes == j), 1.0, 0.0).astype(bf16)
    hidden[...] = dot(h, perm)
    for half, out in enumerate((mine, other)):
        n = 48 * half
        out[HALF:HROWS, :] = jnp.concatenate(
            [hidden[n : n + 24, :], hidden[n + 24 : n + 48, :]], axis=1
        ).astype(bf16)


def down_part(blocks, weights, hidden):
    wa, wb, wc, wd = weights
    c = index("c")
    results = []
    for pair in ((wa, wb), (wc, wd)):
        total = jnp.zeros((HALF, 256), f32)
        shared = jnp.zeros((SHARE, 256), f32)
        for y, *halves in blocks:
            order = pieces(y, c)
            for i, x in enumerate(halves):
                w = [rows_of(pair, DOWN + 128 * p, 128) for p in order[2 * i : 2 * i + 2]]
                total = total + dot(x[0:HALF, :], jnp.concatenate(w, axis=0))
                tail = x[HALF:HROWS, :].astype(f32)
                hidden[48 * i : 48 * i + 24, :] = tail[:, 0:128]
                hidden[48 * i + 24 : 48 * i + 48, :] = tail[:, 128:256]
            w = [
                rows_of(pair, SDOWN + 32 * slice_of(y, core, h), 32)
                for h in range(2)
                for core in range(2)
            ]
            shared = shared + dot(hidden[...].astype(bf16), jnp.concatenate(w, axis=0))
        results.append((total, shared))
    return results


def down_near_body(*refs):
    halves, weights, (products, shared, hidden) = refs[0:6], refs[6:10], refs[10:]
    for i, (a, b) in enumerate(down_part(placed(*halves, None, None)[:3], weights, hidden)):
        products[i] = a
        shared[i] = b


def down_far_body(*refs):
    far, weights, (products, shared), (back, give, skeep, sgive, hidden) = (
        refs[0:2],
        refs[2:6],
        refs[6:8],
        refs[8:],
    )
    parts = down_part(placed(*[None] * 6, *far)[3:], weights, hidden)
    for i, (out, sout) in enumerate(((back.at[index("c")], skeep), (give, sgive))):
        out[...] = (products[i] + parts[i][0]).astype(bf16)
        sout[...] = shared[i] + parts[i][1]


def combine_body(rows, cols, skeep, sother, keep, give, acc):
    yl, c = index("yl"), index("c")
    n = SP * CAP
    slot = lax.broadcasted_iota(i32, (TOK, n), 1).astype(f32)
    meta = cols[...]
    first = dot(jnp.where(slot == meta[:, 0:1], 1.0, 0.0).astype(bf16), rows[...])
    second = dot(jnp.where(slot == meta[:, 1:2], 1.0, 0.0).astype(bf16), rows[...])
    acc[...] = meta[:, 2:3] * first + meta[:, 3:4] * second
    for core, part in ((c, skeep), (1 - c, sother)):
        start = pl.multiple_of((yl * 2 + core) * SHARE, SHARE)
        acc[pl.ds(start, SHARE), :] += part[...]
    keep[...] = acc[:, 0:128]
    give[...] = acc[:, 128:256]


def final_body(stream, keep, other, out):
    out[...] = (stream[...].astype(f32) + keep[...] + other[...]).astype(bf16)


def sds(shape, dtype=bf16):
    return jax.ShapeDtypeStruct(shape, dtype)


def ring(mine, other):
    up = [(i, (i + 1) % 4) for i in range(4)]
    down = [(j, i) for i, j in up]
    up_mine = lax.ppermute(mine, "yh", up)
    down_other = lax.ppermute(other, "yh", down)
    up_other = lax.ppermute(other, "yh", up)
    down_mine = lax.ppermute(mine, "yh", down)
    far_mine = lax.ppermute(up_mine, "yh", up)
    far_other = lax.ppermute(down_other, "yh", down)
    return (mine, other, up_mine, up_other, down_mine, down_other, far_mine, far_other)


def layer(
    outer_gate,
    inner_gate,
    conv_input,
    conv_taps,
    mix_weight,
    residual,
    norm_gain,
    routes,
    route_scores,
    expert_gate,
    expert_up,
    expert_down,
    shared_gate,
    shared_up,
    shared_down,
):
    c = index("c")
    swap = [(0, 1), (1, 0)]
    tp = ("yh", "yl", "c")

    column = sds((32, 1))
    last, begin, product, gate, mine, taps, chosen, scores = call(
        first_body,
        (
            column,
            column,
            sds((32, TOK)),
            sds((32, TOK)),
            sds((MIX + TOK + GAIN, 128)),
            sds((3, 32)),
            sds((2, TOK), i32),
            sds((2, TOK), f32),
        ),
        9,
        [
            pltpu.VMEM((32, TOK), bf16),
            pltpu.VMEM((32, TOK), bf16),
            pltpu.VMEM((1, 128), bf16),
            pltpu.SemaphoreType.DMA((9,)),
        ],
        space=ANY,
        out_space=VM,
    )(
        *(
            pltpu.with_memory_space_constraint(w, pltpu.HBM)
            for w in (
                outer_gate,
                inner_gate,
                conv_input,
                mix_weight,
                residual,
                norm_gain.reshape(1, 128),
                conv_taps,
                routes.T,
                route_scores.T,
            )
        )
    )
    up = [(i, i + 1) for i in range(SP - 1)]
    before = lax.ppermute(last, "sp", up)
    after = lax.ppermute(begin, "sp", [(j, i) for i, j in up])
    near = lax.ppermute(mine, tp, NEAR)

    slots, cols = call(meta_body, (sds((8, TOK), f32), sds((TOK, 128), f32)), 2)(chosen, scores)
    def picked(mine):
        return call(
            functools.partial(pick_body, mine),
            sds((WROWS, 128)),
            6,
            [pltpu.VMEM((D // 2, 128), bf16), pltpu.SemaphoreType.DMA((37,))],
            space=ANY,
        )(
            *(
                pltpu.with_memory_space_constraint(w, pltpu.HBM)
                for w in (expert_gate, expert_up, expert_down, shared_gate.T, shared_up.T, shared_down)
            )
        )

    w_other = picked(False)
    w_own = picked(True)

    mixed = call(mixer_body, sds((32, TOK)), 5)(
        gate, product, taps, before, after
    )
    mixed, near, w_other = lax.optimization_barrier((mixed, near, w_other))
    mixed = lax.all_gather(mixed, tp, axis=0, tiled=True)
    mixed, w_other = lax.optimization_barrier((mixed, w_other))
    w_got = lax.ppermute(w_other, tp, NEAR)
    w_own_c = lax.ppermute(w_own, "c", swap)
    stream, send, shared = call(
        dispatch_body,
        (sds((TOK, 128)), sds((SP * CAP, 256)), sds((2, SHARE + GAIN, 256))),
        4,
        [pltpu.VMEM((TOK, 256), bf16)],
    )(mixed, mine, near, slots)
    arrived = lax.all_to_all(send.reshape(SP, CAP, 256), "sp", 0, 0, tiled=True)
    rows, give = call(split_body, (sds((BLOCK, 256)), sds((BLOCK, 256))), 2)(
        arrived.reshape(SP * CAP, 256), shared
    )
    got = lax.ppermute(give, "c", swap)
    x_ring = ring(rows, got)
    w_got_c = lax.ppermute(w_got, "c", swap)
    weights = (w_own, w_got, w_own_c, w_got_c)

    near_parts = call(
        up_near_body,
        (sds((USED, 128), f32), sds((4, HALF, 256), f32), sds((SHARE, 256), f32)),
        10,
        [pltpu.VMEM((USED, 3 * 512), bf16)],
        limit=16,
    )(*x_ring[:6], *weights)
    hidden = call(
        up_far_body,
        (sds((HROWS, 256)), sds((HROWS, 256))),
        9,
        [pltpu.VMEM((USED, 512), bf16), pltpu.VMEM((SHARE, 128), f32)],
        limit=12,
    )(*x_ring[6:], *weights, *near_parts)
    h_ring = ring(*hidden)
    near_parts = call(
        down_near_body,
        (sds((2, HALF, 256), f32), sds((2, SHARE, 256), f32)),
        10,
        [pltpu.VMEM((SHARE, 128), f32)],
        limit=12,
    )(*h_ring[:6], *weights)
    back, give, skeep, sgive = call(
        down_far_body,
        (sds((2, HALF, 256)), sds((HALF, 256)), sds((SHARE, 256), f32), sds((SHARE, 256), f32)),
        8,
        [pltpu.VMEM((SHARE, 128), f32)],
        limit=12,
    )(*h_ring[6:], *weights, *near_parts)
    got = lax.ppermute(give, "c", swap)
    sgot = lax.ppermute(sgive, "c", swap)
    back = lax.dynamic_update_index_in_dim(back, got, 1 - c, 0)
    back = lax.all_to_all(back.reshape(SP, CAP, 256), "sp", 0, 0, tiled=True)
    keep, other = call(
        combine_body, (sds((TOK, 128), f32), sds((TOK, 128), f32)), 4, [pltpu.VMEM((TOK, 256), f32)]
    )(back.reshape(SP * CAP, 256), cols, skeep, sgot)
    other = lax.ppermute(other, tp, NEAR)
    return call(final_body, sds((TOK, 128)), 3)(stream, keep, other)


def solution(mesh):
    fine = Mesh(mesh.devices.reshape(SP, 4, 2, 2), ("sp", "yh", "yl", "c"))
    tp = ("yh", "yl", "c")
    in_specs = (
        P(tp, "sp"),
        P(tp, "sp"),
        P(tp, "sp"),
        P(None, tp),
        P(None, tp),
        P("sp", tp),
        P(tp),
        P("sp", None),
        P("sp", None),
        P("sp", None, tp),
        P("sp", None, tp),
        P("sp", None, tp),
        P(None, tp),
        P(None, tp),
        P(None, tp),
    )
    return jax.shard_map(
        layer, mesh=fine, in_specs=in_specs, out_specs=P("sp", tp), check_vma=False
    )
```

```python
import functools

import jax
import jax.numpy as jnp
from jax import lax
from jax.experimental import pallas as pl
from jax.experimental.pallas import tpu as pltpu
from jax.sharding import Mesh, PartitionSpec as P


epsilon = 1e-06
routed_scale = 2.5
bf16, f32, i32 = jnp.bfloat16, jnp.float32, jnp.int32

D = 2048
TOK = 384
CAP = 24
SP = 32
EXPERTS = 64
HALF = SP // 2 * CAP
SHARE = TOK // 4
GAIN = 8
MIX = 512
USED = HALF + SHARE
BLOCK = USED + GAIN
HROWS = HALF + SHARE // 4

NEAR = [(2 * y, 2 * (y ^ 1)) for y in range(8)] + [
    (2 * y + 1, 2 * ((y + (1 if y % 2 else 7)) % 8) + 1) for y in range(8)
]
DOWN = 2 * D
PACK = 3 * D
SDOWN = PACK + D // 2
WROWS = SDOWN + 512

VM = pl.BlockSpec(memory_space=pltpu.VMEM)
ANY = pl.BlockSpec(memory_space=pl.ANY)
MIB = 1 << 20


def dot(a, b):
    return lax.dot_general(a, b, (((1,), (0,)), ((), ())), preferred_element_type=f32)


def call(body, outs, count, scratch=(), limit=8, space=VM, out_space=None):
    return pl.pallas_call(
        body,
        out_shape=outs,
        in_specs=[space] * count,
        out_specs=jax.tree.map(lambda _: out_space or space, outs),
        scratch_shapes=scratch,
        compiler_params=pltpu.CompilerParams(vmem_limit_bytes=limit * MIB),
    )


def index(axis):
    return lax.axis_index(axis)


def pick_body(mine, gate, up, down, sg, su, sd, out, pack, sem):
    which = index("yl") if mine else 1 - index("yl")
    copies = [(w.at[which], out.at[pl.ds(i * D, D)]) for i, w in enumerate((gate, up, down))]
    copies.append((sd, out.at[pl.ds(SDOWN, 512)]))
    copies = [pltpu.make_async_copy(a, b, sem.at[i]) for i, (a, b) in enumerate(copies)]
    loads = [
        pltpu.make_async_copy(
            w.at[:, pl.ds(128 * b, 128)], pack.at[pl.ds(64 * b + 32 * i, 32)], sem.at[4 + 16 * i + b]
        )
        for i, w in enumerate((sg, su))
        for b in range(16)
    ]
    for copy in loads + copies:
        copy.start()
    for copy in loads:
        copy.wait()
    store = pltpu.make_async_copy(pack, out.at[pl.ds(PACK, D // 2)], sem.at[36])
    store.start()
    for copy in copies + [store]:
        copy.wait()


def first_body(*refs):
    outer, inner, conv, weight, residual, gain, taps, routes, scores = refs[:9]
    last, begin, product, gate, mine, taps_out, routes_out, scores_out = refs[9:17]
    a, b, g, sem = refs[17:]
    pairs = (
        (inner, a),
        (conv, b),
        (gain, g),
        (outer, gate),
        (weight, mine.at[pl.ds(0, MIX)]),
        (residual, mine.at[pl.ds(MIX, TOK)]),
        (taps, taps_out),
        (routes, routes_out),
        (scores, scores_out),
    )
    copies = [pltpu.make_async_copy(x, y, sem.at[i]) for i, (x, y) in enumerate(pairs)]
    for copy in copies:
        copy.start()
    for copy in copies[:3]:
        copy.wait()
    value = (a[...].astype(f32) * b[...].astype(f32)).astype(bf16)
    last[...] = value[:, TOK - 1 : TOK]
    begin[...] = value[:, 0:1]
    product[...] = value
    mine[MIX + TOK :, :] = jnp.broadcast_to(g[...], (GAIN, 128))
    for copy in copies[3:]:
        copy.wait()


def mixer_body(gate, value, taps, before, after, out):
    product = value[...].astype(f32)
    lane = lax.broadcasted_iota(i32, product.shape, 1)
    left = jnp.where(lane == 0, before[...].astype(f32), pltpu.roll(product, 1, 1))
    right = jnp.where(lane == TOK - 1, after[...].astype(f32), pltpu.roll(product, TOK - 1, 1))
    i = lax.broadcasted_iota(i32, (32, 32), 0)
    j = lax.broadcasted_iota(i32, (32, 32), 1)
    k = taps[...].astype(f32)
    k = [jnp.sum(jnp.where(i == j, k[n : n + 1, :], 0.0), axis=1, keepdims=True) for n in range(3)]
    filtered = k[0] * left + k[1] * product + k[2] * right
    out[...] = (gate[...].astype(f32) * filtered).astype(bf16)


def meta_body(routes, scores, rows_out, cols_out):
    yl = index("yl")
    e = lax.broadcasted_iota(i32, (EXPERTS, TOK), 0)
    m0 = e == routes[0:1, :]
    m1 = e == routes[1:2, :]
    member = jnp.where(m0 | m1, 1.0, 0.0).astype(bf16)
    a = lax.broadcasted_iota(i32, (TOK, TOK), 0)
    b = lax.broadcasted_iota(i32, (TOK, TOK), 1)
    earlier = dot(member, jnp.where(a < b, 1.0, 0.0).astype(bf16))
    base = (lax.shift_right_logical(e, 1) * CAP + 1).astype(f32)
    value = jnp.where((e & 1) == yl, base + earlier, 0.0)
    s0 = jnp.sum(jnp.where(m0, value, 0.0), axis=0, keepdims=True) - 1.0
    s1 = jnp.sum(jnp.where(m1, value, 0.0), axis=0, keepdims=True) - 1.0
    row = lax.broadcasted_iota(i32, (8, TOK), 0)
    rows_out[...] = jnp.where(row == 0, s0, s1)
    total = scores[0:1, :] + scores[1:2, :]
    w0 = scores[0:1, :] / total * routed_scale
    w1 = scores[1:2, :] / total * routed_scale
    row = lax.broadcasted_iota(i32, (128, TOK), 0)
    table = jnp.where(row == 0, s0, jnp.where(row == 1, s1, jnp.where(row == 2, w0, w1)))
    cols_out[...] = table.T


def dispatch_body(mixed, mine, near, slots, stream, send, shared, tokens):
    yl = index("yl")
    weight = jnp.concatenate([mine[0:MIX, :], near[0:MIX, :]], axis=1)
    residual = jnp.concatenate([mine[MIX : MIX + TOK, :], near[MIX : MIX + TOK, :]], axis=1)
    projected = lax.dot_general(
        mixed[...], weight, (((0,), (0,)), ((), ())), preferred_element_type=f32
    )
    tokens[...] = (residual.astype(f32) + projected).astype(bf16)
    stream[...] = tokens[:, 0:128]
    row = lax.broadcasted_iota(i32, (SP * CAP, TOK), 0).astype(f32)
    pick = (row == slots[0:1, :]) | (row == slots[1:2, :])
    send[...] = dot(jnp.where(pick, 1.0, 0.0).astype(bf16), tokens[...]).astype(bf16)
    for core in range(2):
        start = pl.multiple_of((yl * 2 + core) * SHARE, SHARE)
        shared[core, 0:SHARE, :] = tokens[pl.ds(start, SHARE), :]
        for h, x in enumerate((mine, near)):
            shared[core, SHARE : SHARE + GAIN, 128 * h : 128 * h + 128] = x[MIX + TOK :, :]


def silu(v):
    return v * (1.0 / (1.0 + jnp.exp(-v)))


def split_body(arrived, shared, mine, give):
    c = index("c")
    for out, core in ((mine, c), (give, 1 - c)):
        out[0:HALF, :] = arrived[pl.ds(pl.multiple_of(core * HALF, HALF), HALF), :]
        out[HALF:, :] = shared[core]


def placed(mine, other, up_mine, up_other, down_mine, down_other, far_mine, far_other):
    yh, yl = index("yh"), index("yl")
    return (
        (2 * yh + yl, mine, other),
        (2 * ((yh + 3) % 4) + yl, up_mine, up_other),
        (2 * ((yh + 1) % 4) + yl, down_mine, down_other),
        (2 * ((yh + 2) % 4) + yl, far_mine, far_other),
    )


def slice_of(y, core, near):
    if near:
        yl = index("yl")
        y = jnp.where(core == 1, (y + 2 * yl + 7) % 8, y + 1 - 2 * yl)
    return 2 * y + core


def rows_of(weights, first, count):
    n = pl.multiple_of(first, 32)
    return jnp.concatenate([w[pl.ds(n, count), :] for w in weights], axis=1)


def pieces(y, c):
    return [slice_of(y, core, h) for core in (c, 1 - c) for h in range(2)]


def up_part(blocks, weights, scaled, squares):
    wa, wb, wc, wd = weights
    c = index("c")
    for n, (y, *halves) in enumerate(blocks):
        for i, x in enumerate(halves):
            for h in range(2):
                lanes = slice(128 * h, 128 * h + 128)
                v = x[0:USED, lanes].astype(f32)
                squares = squares + v * v
                gain = x[USED:BLOCK, lanes].astype(f32)[0:1, :]
                at = 512 * n + 256 * i + 128 * h
                scaled[:, at : at + 128] = (v * gain).astype(bf16)
    results = []
    for pair in ((wa, wb), (wc, wd)):
        for base in (0, D):
            total = jnp.zeros((HALF, 256), f32)
            for n, (y, *_) in enumerate(blocks):
                w = [rows_of(pair, base + 128 * p, 128) for p in pieces(y, c)]
                x = scaled[0:HALF, 512 * n : 512 * n + 512]
                total = total + dot(x, jnp.concatenate(w, axis=0))
            results.append(total)
    shared = jnp.zeros((SHARE, 256), f32)
    for n, (y, *_) in enumerate(blocks):
        packed = jnp.concatenate(
            [
                jnp.concatenate([rows_of([w], PACK + 64 * p, 64) for p in pieces(y, c)], axis=1)
                for w in (wa, wc, wb, wd)
            ],
            axis=0,
        )
        x = scaled[HALF:USED, 512 * n : 512 * n + 512]
        shared = shared + lax.dot_general(
            x, packed, (((1,), (1,)), ((), ())), preferred_element_type=f32
        )
    return squares, results, shared


def up_near_body(*refs):
    halves, weights, (squares, products, shared, scaled) = refs[0:6], refs[6:10], refs[10:]
    blocks = placed(*halves, None, None)[:3]
    total, results, part = up_part(blocks, weights, scaled, jnp.zeros((USED, 128), f32))
    squares[...] = total
    for i, value in enumerate(results):
        products[i] = value
    shared[...] = part


def up_far_body(*refs):
    far, weights, (squares, products, shared), (mine, other, scaled, hidden) = (
        refs[0:2],
        refs[2:6],
        refs[6:9],
        refs[9:],
    )
    c = index("c")
    blocks = placed(*[None] * 6, *far)[3:]
    total, results, part = up_part(blocks, weights, scaled, squares[...])
    inverse = lax.rsqrt(jnp.sum(total, axis=1, keepdims=True) / D + epsilon)
    rows = inverse[0:HALF]
    for i, out in enumerate((mine, other)):
        g = (products[2 * i] + results[2 * i]) * rows
        u = (products[2 * i + 1] + results[2 * i + 1]) * rows
        out[0:HALF, :] = (silu(g) * u).astype(bf16)
    s = (shared[...] + part) * inverse[HALF:]
    h = (silu(s) * pltpu.roll(s, 256 - 32, 1)).astype(bf16)
    i = lax.broadcasted_iota(i32, (256, 128), 0)
    j = lax.broadcasted_iota(i32, (256, 128), 1)
    goes = (lax.shift_right_logical(i, 6) * 32 + (i & 31)) ^ (c * 32)
    perm = jnp.where(((i & 32) == 0) & (goes == j), 1.0, 0.0).astype(bf16)
    hidden[...] = dot(h, perm)
    for half, out in enumerate((mine, other)):
        n = 48 * half
        out[HALF:HROWS, :] = jnp.concatenate(
            [hidden[n : n + 24, :], hidden[n + 24 : n + 48, :]], axis=1
        ).astype(bf16)


def down_part(blocks, weights, hidden):
    wa, wb, wc, wd = weights
    c = index("c")
    results = []
    for pair in ((wa, wb), (wc, wd)):
        total = jnp.zeros((HALF, 256), f32)
        shared = jnp.zeros((SHARE, 256), f32)
        for y, *halves in blocks:
            order = pieces(y, c)
            for i, x in enumerate(halves):
                w = [rows_of(pair, DOWN + 128 * p, 128) for p in order[2 * i : 2 * i + 2]]
                total = total + dot(x[0:HALF, :], jnp.concatenate(w, axis=0))
                tail = x[HALF:HROWS, :].astype(f32)
                hidden[48 * i : 48 * i + 24, :] = tail[:, 0:128]
                hidden[48 * i + 24 : 48 * i + 48, :] = tail[:, 128:256]
            w = [
                rows_of(pair, SDOWN + 32 * slice_of(y, core, h), 32)
                for h in range(2)
                for core in range(2)
            ]
            shared = shared + dot(hidden[...].astype(bf16), jnp.concatenate(w, axis=0))
        results.append((total, shared))
    return results


def down_near_body(*refs):
    halves, weights, (products, shared, hidden) = refs[0:6], refs[6:10], refs[10:]
    for i, (a, b) in enumerate(down_part(placed(*halves, None, None)[:3], weights, hidden)):
        products[i] = a
        shared[i] = b


def down_far_body(*refs):
    far, weights, (products, shared), (back, give, skeep, sgive, hidden) = (
        refs[0:2],
        refs[2:6],
        refs[6:8],
        refs[8:],
    )
    parts = down_part(placed(*[None] * 6, *far)[3:], weights, hidden)
    for i, (out, sout) in enumerate(((back.at[index("c")], skeep), (give, sgive))):
        out[...] = (products[i] + parts[i][0]).astype(bf16)
        sout[...] = shared[i] + parts[i][1]


def combine_body(rows, cols, skeep, sother, keep, give, acc):
    yl, c = index("yl"), index("c")
    n = SP * CAP
    slot = lax.broadcasted_iota(i32, (TOK, n), 1).astype(f32)
    meta = cols[...]
    first = dot(jnp.where(slot == meta[:, 0:1], 1.0, 0.0).astype(bf16), rows[...])
    second = dot(jnp.where(slot == meta[:, 1:2], 1.0, 0.0).astype(bf16), rows[...])
    acc[...] = meta[:, 2:3] * first + meta[:, 3:4] * second
    for core, part in ((c, skeep), (1 - c, sother)):
        start = pl.multiple_of((yl * 2 + core) * SHARE, SHARE)
        acc[pl.ds(start, SHARE), :] += part[...]
    keep[...] = acc[:, 0:128]
    give[...] = acc[:, 128:256].astype(bf16)


def final_body(stream, keep, other, out):
    out[...] = (stream[...].astype(f32) + keep[...] + other[...].astype(f32)).astype(bf16)


def sds(shape, dtype=bf16):
    return jax.ShapeDtypeStruct(shape, dtype)


def ring(mine, other):
    up = [(i, (i + 1) % 4) for i in range(4)]
    down = [(j, i) for i, j in up]
    up_mine = lax.ppermute(mine, "yh", up)
    down_other = lax.ppermute(other, "yh", down)
    up_other = lax.ppermute(other, "yh", up)
    down_mine = lax.ppermute(mine, "yh", down)
    far_mine = lax.ppermute(up_mine, "yh", up)
    far_other = lax.ppermute(down_other, "yh", down)
    return (mine, other, up_mine, up_other, down_mine, down_other, far_mine, far_other)


def layer(
    outer_gate,
    inner_gate,
    conv_input,
    conv_taps,
    mix_weight,
    residual,
    norm_gain,
    routes,
    route_scores,
    expert_gate,
    expert_up,
    expert_down,
    shared_gate,
    shared_up,
    shared_down,
):
    c = index("c")
    swap = [(0, 1), (1, 0)]
    tp = ("yh", "yl", "c")

    column = sds((32, 1))
    last, begin, product, gate, mine, taps, chosen, scores = call(
        first_body,
        (
            column,
            column,
            sds((32, TOK)),
            sds((32, TOK)),
            sds((MIX + TOK + GAIN, 128)),
            sds((3, 32)),
            sds((2, TOK), i32),
            sds((2, TOK), f32),
        ),
        9,
        [
            pltpu.VMEM((32, TOK), bf16),
            pltpu.VMEM((32, TOK), bf16),
            pltpu.VMEM((1, 128), bf16),
            pltpu.SemaphoreType.DMA((9,)),
        ],
        space=ANY,
        out_space=VM,
    )(
        *(
            pltpu.with_memory_space_constraint(w, pltpu.HBM)
            for w in (
                outer_gate,
                inner_gate,
                conv_input,
                mix_weight,
                residual,
                norm_gain.reshape(1, 128),
                conv_taps,
                routes.T,
                route_scores.T,
            )
        )
    )
    up = [(i, i + 1) for i in range(SP - 1)]
    before = lax.ppermute(last, "sp", up)
    after = lax.ppermute(begin, "sp", [(j, i) for i, j in up])
    near = lax.ppermute(mine, tp, NEAR)

    slots, cols = call(meta_body, (sds((8, TOK), f32), sds((TOK, 128), f32)), 2)(chosen, scores)
    def picked(mine):
        return call(
            functools.partial(pick_body, mine),
            sds((WROWS, 128)),
            6,
            [pltpu.VMEM((D // 2, 128), bf16), pltpu.SemaphoreType.DMA((37,))],
            space=ANY,
        )(
            *(
                pltpu.with_memory_space_constraint(w, pltpu.HBM)
                for w in (expert_gate, expert_up, expert_down, shared_gate.T, shared_up.T, shared_down)
            )
        )

    w_other = picked(False)
    w_own = picked(True)

    mixed = call(mixer_body, sds((32, TOK)), 5)(
        gate, product, taps, before, after
    )
    mixed, near, w_other, slots, cols = lax.optimization_barrier(
        (mixed, near, w_other, slots, cols)
    )
    mixed = lax.all_gather(mixed, tp, axis=0, tiled=True)
    mixed, w_other = lax.optimization_barrier((mixed, w_other))
    w_got = lax.ppermute(w_other, tp, NEAR)
    w_own_c = lax.ppermute(w_own, "c", swap)
    stream, send, shared = call(
        dispatch_body,
        (sds((TOK, 128)), sds((SP * CAP, 256)), sds((2, SHARE + GAIN, 256))),
        4,
        [pltpu.VMEM((TOK, 256), bf16)],
    )(mixed, mine, near, slots)
    arrived = lax.all_to_all(send.reshape(SP, CAP, 256), "sp", 0, 0, tiled=True)
    rows, give = call(split_body, (sds((BLOCK, 256)), sds((BLOCK, 256))), 2)(
        arrived.reshape(SP * CAP, 256), shared
    )
    got = lax.ppermute(give, "c", swap)
    x_ring = ring(rows, got)
    w_got_c = lax.ppermute(w_got, "c", swap)
    weights = (w_own, w_got, w_own_c, w_got_c)

    near_parts = call(
        up_near_body,
        (sds((USED, 128), f32), sds((4, HALF, 256), f32), sds((SHARE, 256), f32)),
        10,
        [pltpu.VMEM((USED, 3 * 512), bf16)],
        limit=16,
    )(*x_ring[:6], *weights)
    hidden = call(
        up_far_body,
        (sds((HROWS, 256)), sds((HROWS, 256))),
        9,
        [pltpu.VMEM((USED, 512), bf16), pltpu.VMEM((SHARE, 128), f32)],
        limit=12,
    )(*x_ring[6:], *weights, *near_parts)
    h_ring = ring(*hidden)
    near_parts = call(
        down_near_body,
        (sds((2, HALF, 256), f32), sds((2, SHARE, 256), f32)),
        10,
        [pltpu.VMEM((SHARE, 128), f32)],
        limit=12,
    )(*h_ring[:6], *weights)
    back, give, skeep, sgive = call(
        down_far_body,
        (sds((2, HALF, 256)), sds((HALF, 256)), sds((SHARE, 256), f32), sds((SHARE, 256), f32)),
        8,
        [pltpu.VMEM((SHARE, 128), f32)],
        limit=12,
    )(*h_ring[6:], *weights, *near_parts)
    got = lax.ppermute(give, "c", swap)
    sgot = lax.ppermute(sgive, "c", swap)
    back = lax.dynamic_update_index_in_dim(back, got, 1 - c, 0)
    back = lax.all_to_all(back.reshape(SP, CAP, 256), "sp", 0, 0, tiled=True)
    keep, other = call(
        combine_body, (sds((TOK, 128), f32), sds((TOK, 128))), 4, [pltpu.VMEM((TOK, 256), f32)]
    )(back.reshape(SP * CAP, 256), cols, skeep, sgot)
    other = lax.ppermute(other, tp, NEAR)
    return call(final_body, sds((TOK, 128)), 3)(stream, keep, other)


def solution(mesh):
    fine = Mesh(mesh.devices.reshape(SP, 4, 2, 2), ("sp", "yh", "yl", "c"))
    tp = ("yh", "yl", "c")
    in_specs = (
        P(tp, "sp"),
        P(tp, "sp"),
        P(tp, "sp"),
        P(None, tp),
        P(None, tp),
        P("sp", tp),
        P(tp),
        P("sp", None),
        P("sp", None),
        P("sp", None, tp),
        P("sp", None, tp),
        P("sp", None, tp),
        P(None, tp),
        P(None, tp),
        P(None, tp),
    )
    return jax.shard_map(
        layer, mesh=fine, in_specs=in_specs, out_specs=P("sp", tp), check_vma=False
    )
```
